256 devices in a mesh: sp: 64 (over z, y, core), tp: 4 (over x).
Axes of the slice: x: 4, y: 4, z: 8, core: 2. Of those that a mesh axis runs over, the one named last changes fastest.
Arguments:
- residual: bfloat16 [4, 6144, 2048], P('tp', 'sp'), may hold values from -3 to 3
- query_nope: bfloat16 [4, 6144, 1024], P('tp', 'sp'), may hold values from -9 to 9
- query_rope: bfloat16 [4, 6144, 512], P('tp', 'sp'), may hold values from -48 to 48
- latent: bfloat16 [4, 6144, 128], P('tp', 'sp'), may hold values from -6 to 6
- rope_key: bfloat16 [4, 6144, 32], P('tp', 'sp'), may hold values from -48 to 48
- latent_gain: float32 [128], replicated, may hold values from 0.1 to 1.9
- up_key: bfloat16 [128, 1024], replicated, may hold values from -1 to 1
- up_value: bfloat16 [128, 1024], replicated, may hold values from -0.5 to 0.5
- out_weight: bfloat16 [1024, 2048], replicated, may hold values from -0.375 to 0.375
- ffn_gain: float32 [2048], replicated, may hold values from 0.1 to 1.9
- routes: int32 [4, 6144, 2], P(None, 'sp'), may hold values from 0 to 63, all different within a row; in each aligned block of 96 rows (0 to 95, 96 to 191, ..., all dimensions but the last counted through in order) at most 3 rows name the same one
- route_weight: float32 [4, 6144, 2], P('tp', 'sp'), may hold values from 0.1 to 1
- gate_weight: bfloat16 [64, 2048, 1024], P('sp', None, 'tp'), may hold values from -1.5 to 1.5
- up_weight: bfloat16 [64, 2048, 1024], P('sp', None, 'tp'), may hold values from -1.5 to 1.5
- down_weight: bfloat16 [64, 1024, 2048], P('sp', 'tp'), may hold values from -0.046875 to 0.046875
Outputs:
- updated: bfloat16 [4, 6144, 2048], P('tp', 'sp')
The draws below stay inside these ranges and needn't reach their ends.
Inputs may be any that keep to these rules, and one draw needn't show every extreme that they name: `routes`: each row names 2 different experts. In each aligned block of 96 rows (one sequence's rows of one device) no expert is named by more than 3 rows, a bound that some block reaches.
All inputs are finite; a program needn't handle non-finite values.
Results may differ from the reference program's by a relative error of at most 0.017.
Values may be sent and summed in bfloat16 or wider, within the bound.
A program may use at most 64 MiB of HBM per device.

```python
import math
import jax
import jax.numpy as jnp
import numpy as np
from jax import lax

D = 2048
HEADS = 16
NOPE = 64
ROPE = 32
VDIM = 64
LATENT = 128
FF = 1024
TOPK = 2
TOK_DEV = 96
SEQS = 4
LENGTH = 6144
EXPERTS = 64
FF_BLOCK = 256
MOST = 3
N_SP = 64
N_TP = 4


def rope_pair(key):
    base = jax.random.fold_in(key, 7)
    shape_keys = (SEQS, LENGTH, ROPE)
    shape_queries = (SEQS, LENGTH, HEADS, ROPE)
    keys = jax.random.normal(jax.random.fold_in(base, 1), shape_keys, jnp.float32) * 1.5
    queries = jax.random.normal(jax.random.fold_in(base, 2), shape_queries, jnp.float32) * 1.5
    return (keys, queries.reshape(SEQS, LENGTH, HEADS * ROPE))


def expert_matrix(key, salt):
    base = jax.random.fold_in(key, salt)
    values = jax.random.normal(jax.random.fold_in(base, 1), (EXPERTS, D, FF), jnp.float32)
    columns = jnp.exp(jax.random.uniform(jax.random.fold_in(base, 2), (EXPERTS, 1, FF), jnp.float32, math.log(0.5), math.log(6.0)))
    return jnp.clip(values * columns * D ** (-0.5), -1.5, 1.5)


def draw_query_rope(key, part):
    return rope_pair(key)[1].astype(jnp.bfloat16)


def draw_rope_key(key, part):
    return rope_pair(key)[0].astype(jnp.bfloat16)


def draw_gate_weight(key, part):
    return expert_matrix(key, 101).astype(jnp.bfloat16)


def draw_up_weight(key, part):
    return expert_matrix(key, 202).astype(jnp.bfloat16)


def level_of(stream_key, shape, shards, low, high):
    level, own = 1.0, jax.random.fold_in(stream_key, 6)
    for dim, shards_of in shards:
        steps = jnp.exp(jax.random.uniform(jax.random.fold_in(own, dim), (shards_of,), jnp.float32, low / len(shards), high / len(shards)))
        level = level * jnp.repeat(steps, shape[dim] // shards_of).reshape([-1 if axis == dim else 1 for axis in range(len(shape))])
    return level


def shared_out(own_key, own, number, rows, amount, top, limit, lean):
    order = jax.random.permutation(own_key, amount)
    packed, ordinary = load_shares(amount, rows * top, limit, lean, True), load_shares(amount, rows * top, limit, lean, False)
    places = jnp.arange(amount)

    def named(tallies, offset_by):
        used = int((tallies > 0).sum())
        fixed = max(1, used // 4)
        passed = fixed + (places - fixed + offset_by * (used - fixed)) % max(1, amount - fixed)
        return jnp.zeros((amount,), jnp.int32).at[order[jnp.where(places < fixed, places, passed)]].set(jnp.asarray(tallies, jnp.int32))

    tallies = jnp.where(number % 4 == 0, named(packed, number // 4), named(ordinary, number - number // 4 - 1))
    mixed = jax.random.permutation(jax.random.fold_in(own, 3), amount)
    giver, sink = mixed[0:amount // 2 * 2:2], mixed[1:amount // 2 * 2:2]
    room = jnp.minimum(tallies[giver] - 1, limit - tallies[sink]) // 2
    room = jnp.where((giver == order[0]) | (sink == order[0]) | (tallies[sink] == 0), 0, jnp.maximum(room, 0))
    passed = jax.random.randint(jax.random.fold_in(own, 4), (amount // 2,), 0, 1 << 20) % (room + 1)
    tallies = tallies.at[giver].add(-passed).at[sink].add(passed)
    members = jnp.searchsorted(jnp.cumsum(tallies), jnp.arange(rows * top), side="right").astype(jnp.int32)
    grid = members.reshape(top, rows).T
    grid = grid[jax.random.permutation(jax.random.fold_in(own, 1), rows)]
    offset_by = jax.random.randint(jax.random.fold_in(own, 2), (rows, 1), 0, top)
    return jnp.take_along_axis(grid, (jnp.arange(top)[None, :] + offset_by) % top, axis=1)


def load_shares(count, total, reach, skew, full):
    portions = [(1 << 20) // math.isqrt(standing ** skew) + 1 for standing in range(1, count + 1)]
    largest = reach if full else min(reach, max(-(-total // count), total * portions[0] // sum(portions)))
    least = 1 if total - largest >= count - 1 else 0
    given, rest = [largest] + [least] * (count - 1), total - largest - least * (count - 1)
    while rest > 0:
        candidates = [i for i in range(1, count) if given[i] < largest] or [i for i in range(1, count) if given[i] < reach]
        whole, budget = sum([portions[i] for i in candidates]), rest
        for i in candidates:
            addition = min(reach - given[i], max(1, budget * portions[i] // whole), rest)
            given[i] = given[i] + addition
            rest = rest - addition
    return np.array(given)


def bell_draw(own_key, dims, spread, most, shards=(), held_as=jnp.bfloat16):
    loudness = level_of(own_key, dims, shards, -0.22, 0.18) if shards else 1.0
    values = jax.random.normal(own_key, dims, jnp.float32) * spread * loudness
    return jnp.minimum(jnp.maximum(values, -most), most).astype(held_as)


def setup_inputs(seed: int = 0) -> dict:
    key_list = jax.random.split(jax.random.key(seed), 16)
    residual = bell_draw(key_list[0], (SEQS, LENGTH, D), 0.5, 3.0, ((0, 4), (1, 64)))
    query_nope = bell_draw(key_list[1], (SEQS, LENGTH, HEADS * NOPE), 1.5, 9.0, ((0, 4), (1, 64)))
    query_rope = draw_query_rope(jax.random.fold_in(key_list[15], 71), 0)
    latent = bell_draw(key_list[3], (SEQS, LENGTH, LATENT), 1.0, 6.0, ((0, 4), (1, 64)))
    rope_key = draw_rope_key(jax.random.fold_in(key_list[15], 71), 0)
    latent_gain = jnp.clip(1.0 + 0.18 * jax.random.normal(key_list[5], (LATENT,), jnp.float32), 0.1, 1.9)
    up_key = bell_draw(key_list[6], (LATENT, HEADS * NOPE), (LATENT // 3) ** -0.5, 1.0)
    up_value = bell_draw(key_list[7], (LATENT, HEADS * VDIM), LATENT ** -0.5, 0.5)
    out_weight = bell_draw(key_list[8], (HEADS * VDIM, D), (HEADS * VDIM // 4) ** -0.5, 0.375)
    ffn_gain = jnp.clip(1.0 + 0.18 * jax.random.normal(key_list[9], (D,), jnp.float32), 0.1, 1.9)
    routes_keys = jax.random.split(jax.random.fold_in(key_list[10], 1), SEQS * LENGTH // TOK_DEV)
    routes_turns = jax.random.permutation(jax.random.fold_in(key_list[10], 3), SEQS * LENGTH // TOK_DEV)
    routes = jax.vmap(lambda own, number: shared_out(jax.random.fold_in(key_list[10], 2), own, number, TOK_DEV, EXPERTS, TOPK, MOST, 0))(routes_keys, routes_turns).reshape((SEQS, LENGTH, TOPK))
    route_weight = jnp.clip(jnp.exp(math.log(1.0) - 2.3025851 * jax.random.uniform(key_list[11], (SEQS, LENGTH, TOPK), jnp.float32) ** level_of(key_list[11], (SEQS, LENGTH, TOPK), ((0, 4), (1, 64)), -0.2, 0.2)), 0.1, 1.0)
    gate_weight = draw_gate_weight(jax.random.fold_in(key_list[15], 71), 0)
    up_weight = draw_up_weight(jax.random.fold_in(key_list[15], 71), 0)
    down_weight = bell_draw(key_list[14], (EXPERTS, FF, D), (FF * 16) ** -0.5, 0.046875, ((0, 64), (1, 4)))
    return dict(residual=residual, query_nope=query_nope, query_rope=query_rope, latent=latent, rope_key=rope_key, latent_gain=latent_gain, up_key=up_key, up_value=up_value, out_weight=out_weight, ffn_gain=ffn_gain, routes=routes, route_weight=route_weight, gate_weight=gate_weight, up_weight=up_weight, down_weight=down_weight)


EPS = 1e-06
ROPE_BASE = 10000.0
CLAMP = 7.0
ALPHA = 1.702

def rotate(values, positions, width):
    half = width // 2
    inverse = ROPE_BASE ** (-jnp.arange(half, dtype=jnp.float32) * 2.0 / width)
    angle = positions.astype(jnp.float32)[:, None] * inverse[None, :]
    cosine = jnp.cos(angle)[:, None, :]
    sine = jnp.sin(angle)[:, None, :]
    first = values[..., :half]
    second = values[..., half:]
    return jnp.concatenate([first * cosine - second * sine, first * sine + second * cosine], axis=-1)

def rms_scaled(values, gain):
    return values * lax.rsqrt(lax.optimization_barrier(jnp.mean(values * values, axis=-1, keepdims=True)) + EPS) * gain

def reference(residual, query_nope, query_rope, latent, rope_key, latent_gain, up_key, up_value, out_weight, ffn_gain, routes, route_weight, gate_weight, up_weight, down_weight):
    sequences, length, width = residual.shape
    positions = jnp.arange(length, dtype=jnp.int32)
    factor = (NOPE + ROPE) ** (-0.5)
    normed = rms_scaled(latent.astype(jnp.float32), latent_gain).astype(jnp.bfloat16)
    flat_latent = normed.reshape(-1, LATENT)
    key_part = jnp.dot(flat_latent, up_key, preferred_element_type=jnp.float32).astype(jnp.bfloat16)
    key_part = key_part.reshape(sequences, length, HEADS, NOPE)
    value_part = jnp.dot(flat_latent, up_value, preferred_element_type=jnp.float32).astype(jnp.bfloat16)
    value_part = value_part.reshape(sequences, length, HEADS, VDIM)
    key_turned = rotate(rope_key.astype(jnp.float32)[:, :, None, :], positions, ROPE)[:, :, 0, :].astype(jnp.bfloat16)
    query_turned = rotate(query_rope.astype(jnp.float32).reshape(sequences, length, HEADS, ROPE), positions, ROPE).astype(jnp.bfloat16)
    query_plain = query_nope.reshape(sequences, length, HEADS, NOPE)
    span = math.gcd(length, 256)
    count = length // span

    def one_sequence(items):
        plain, turned, keys, turned_keys, values = items
        keys_wide = keys.astype(jnp.float32)
        turned_wide = turned_keys.astype(jnp.float32)
        values_wide = values.astype(jnp.float32)

        def one_block(pair):
            scores = (jnp.einsum('qhd,khd->hqk', pair[0].astype(jnp.float32), keys_wide) + jnp.einsum('qhd,kd->hqk', pair[1].astype(jnp.float32), turned_wide)) * factor
            peak = lax.optimization_barrier(jnp.max(scores, axis=-1, keepdims=True))
            weights = jnp.exp(scores - peak)
            total = lax.optimization_barrier(jnp.sum(weights, axis=-1))
            rounded = lax.optimization_barrier(weights.astype(jnp.bfloat16)).astype(jnp.float32)
            mixed = jnp.einsum('hqk,khd->qhd', rounded, values_wide)
            return (mixed / jnp.transpose(total)[:, :, None]).astype(jnp.bfloat16)
        blocks = lax.map(one_block, (plain.reshape(count, span, HEADS, NOPE), turned.reshape(count, span, HEADS, ROPE)))
        return blocks.reshape(length, HEADS * VDIM)
    attended = lax.map(one_sequence, (query_plain, query_turned, key_part, key_turned, value_part))
    projected = jnp.dot(attended.reshape(-1, HEADS * VDIM), out_weight, preferred_element_type=jnp.float32)
    middle = (residual.reshape(-1, width).astype(jnp.float32) + projected).astype(jnp.bfloat16)
    middle_wide = lax.optimization_barrier(middle).astype(jnp.float32)
    normal_rows = rms_scaled(middle_wide, ffn_gain).astype(jnp.bfloat16)
    total_rows = sequences * length
    flat_picks = routes.reshape(-1)
    flat_weights = route_weight.reshape(-1)
    owner = jnp.arange(total_rows * TOPK, dtype=jnp.int32) // TOPK
    capacity = sequences * N_SP * MOST
    padded = jnp.concatenate([normal_rows, jnp.zeros((1, width), jnp.bfloat16)], axis=0)

    def one_expert(accum, items):
        gate_w, up_w, down_w, index = items
        hit = flat_picks == index
        rank = jnp.cumsum(hit.astype(jnp.int32)) - 1
        slot = jnp.where(hit, rank, capacity).astype(jnp.int32)
        source = jnp.full((capacity + 1,), total_rows, jnp.int32).at[slot].set(owner)[:capacity]
        scale_rows = jnp.zeros((capacity + 1,), jnp.float32).at[slot].set(flat_weights)[:capacity]
        rows = padded[source]
        gate = jnp.minimum(jnp.dot(rows, gate_w, preferred_element_type=jnp.float32), CLAMP)
        lift = jnp.clip(jnp.dot(rows, up_w, preferred_element_type=jnp.float32), -CLAMP, CLAMP)
        active = (gate * jax.nn.sigmoid(ALPHA * gate) * (lift + 1.0)).astype(jnp.bfloat16)
        parts = jnp.einsum('rjf,jfd->jrd', active.reshape(capacity, N_TP, FF_BLOCK).astype(jnp.float32), down_w.reshape(N_TP, FF_BLOCK, width).astype(jnp.float32))
        output = lax.optimization_barrier(jnp.sum(lax.optimization_barrier(parts.astype(jnp.bfloat16)).astype(jnp.float32), axis=0))
        output = output.astype(jnp.bfloat16)
        accum = accum.at[source].add(output.astype(jnp.float32) * scale_rows[:, None])
        return (accum, None)
    accum, _ = lax.scan(one_expert, jnp.zeros((total_rows + 1, width), jnp.float32), (gate_weight, up_weight, down_weight, jnp.arange(EXPERTS, dtype=jnp.int32)))
    updated = (middle_wide + accum[:total_rows]).astype(jnp.bfloat16)
    return updated.reshape(sequences, length, width)
```

```python
import math

import jax
import jax.numpy as jnp
from jax import lax
from jax.experimental import pallas as pl
from jax.experimental.pallas import tpu as pltpu
from jax.sharding import Mesh
from jax.sharding import PartitionSpec as P

HEADS = 16
NOPE = 64
ROPE = 32
VDIM = 64
LATENT = 128
TOPK = 2
SP = ("sp_0", "sp_1", "sp_2")

EPS = 1e-06
ROPE_BASE = 10000.0
CLAMP = 7.0
ALPHA = 1.702
NEG_BIG = -1e30
MESH = pl.DeviceIdType.MESH

F32 = jnp.float32
BF16 = jnp.bfloat16
NZ, NY = 8, 4
TOK = 96
GROUP = NZ * TOK
QROWS = HEADS * TOK
CHUNK = 512
VROWS = LATENT + 16
Z_ORDER = (1, 7, 2, 6, 3, 5, 4)


def gather_axes(x, axes, dim):
    if not axes:
        return x
    nearer = lax.all_gather(x, axes[-1], axis=dim, tiled=True)
    return gather_axes(nearer, axes[:-1], dim)


def laid_out(pieces, dim):
    pieces = jnp.moveaxis(pieces, 0, dim)
    shape = pieces.shape
    return pieces.reshape(*shape[:dim], shape[dim] * shape[dim + 1], *shape[dim + 2 :])


def on_gathered_pieces(x, axis, dim, work, out_dim):
    width = x.shape[dim]
    pieces = jnp.split(x, 2, axis=dim) if width % 2 == 0 else [x]
    initial = jnp.arange(lax.axis_size(axis)) * width
    blocks = [lax.all_gather(section, axis) for section in pieces]
    made = [jax.vmap(work)(b, initial + k * (width // len(pieces))) for k, b in enumerate(blocks)]
    return laid_out(jnp.concatenate(made, axis=out_dim + 1), out_dim)


def split_up(x, dim, size):
    before, after = (x.shape[:dim], x.shape[dim + 1 :])
    return jnp.moveaxis(x.reshape(*before, size, -1, *after), dim, 0)


def sent_and_summed(x, axis, dim):
    size = lax.axis_size(axis)
    pieces = lax.all_to_all(split_up(x, dim, size), axis, 0, 0, tiled=True)
    return jnp.sum(pieces.astype(jnp.float32), axis=0)


def expert_term(rows, gate_w, up_w, down_w):
    gate = jnp.minimum(jnp.dot(rows, gate_w, preferred_element_type=jnp.float32), CLAMP)
    lift = jnp.clip(jnp.dot(rows, up_w, preferred_element_type=jnp.float32), -CLAMP, CLAMP)
    active = (gate * jax.nn.sigmoid(ALPHA * gate) * (lift + 1.0)).astype(jnp.bfloat16)
    return jnp.dot(active, down_w, preferred_element_type=jnp.float32)


def assign(picks, slots, count):
    flat = picks.reshape(-1)
    hot = (flat[:, None] == jnp.arange(count, dtype=jnp.int32)[None, :]).astype(jnp.int32)
    ranks = jnp.sum((jnp.cumsum(hot, axis=0) - 1) * hot, axis=1)
    return flat * slots + ranks


def pack_rows(rows, target, slots, count):
    tokens = rows.shape[0]
    owner = jnp.arange(target.shape[0], dtype=jnp.int32) // (target.shape[0] // tokens)
    source = jnp.full((count * slots,), tokens, jnp.int32).at[target].set(owner)
    padded = jnp.concatenate([rows, jnp.zeros((1, rows.shape[1]), rows.dtype)], axis=0)
    return padded[source]


def nt_dot(a, b):
    return lax.dot_general(a, b, (((1,), (1,)), ((), ())), preferred_element_type=F32)


def iota(shape, dim):
    return lax.broadcasted_iota(jnp.int32, shape, dim)


def turned(x, cosine, sine):
    low = iota(x.shape, 1) % ROPE < ROPE // 2
    swapped = jnp.where(low, pltpu.roll(x, 128 - ROPE // 2, 1), pltpu.roll(x, ROPE // 2, 1))
    return x * cosine + swapped * sine


def attention_kernel(
    qn_ref, qr_ref, lat_ref, key_ref, cos_ref, sin_ref, gain_ref, upk_ref, upv_ref,
    res_ref, fgain_ref, ow_hbm,
    mid_ref, rows_ref,
    held, q_ref, k_ref, v_ref, s_ref, p_ref, acc_ref, peak_ref, ow_ref,
    own_send, fwd_send, pair_send, z_recv, y_recv, pair_recv, ow_sem,
):
    z, y, c = (lax.axis_index(name) for name in SP)
    barrier = pltpu.get_barrier_semaphore()

    def z_peer(d):
        return {"sp_0": lax.rem(z + d, NZ)}

    def y_peer(d):
        return {"sp_1": lax.rem(y + d, NY)}

    partner = {"sp_2": 1 - c}
    for d in range(1, NZ):
        pl.semaphore_signal(barrier, inc=1, device_id=z_peer(d), device_id_type=MESH)
    for d in range(1, NY):
        pl.semaphore_signal(barrier, inc=1, device_id=y_peer(d), device_id_type=MESH)
    pl.semaphore_signal(barrier, inc=1, device_id=partner, device_id_type=MESH)
    ow_copy = pltpu.make_async_copy(ow_hbm, ow_ref, ow_sem)
    ow_copy.start()

    wide = lat_ref[...].astype(F32)
    scale = lax.rsqrt(jnp.mean(wide * wide, axis=-1, keepdims=True) + EPS)
    held[c, y, z, :TOK, :] = (wide * scale * gain_ref[...]).astype(BF16)
    held[c, y, z, TOK:, :] = turned(
        key_ref[...].astype(F32), cos_ref[TOK:, :], sin_ref[TOK:, :]
    ).astype(BF16)

    pl.semaphore_wait(barrier, NZ + NY - 1)

    def to_y(block):
        for d in (1, 3, 2):
            pltpu.make_async_remote_copy(
                src_ref=block, dst_ref=block, send_sem=fwd_send, recv_sem=y_recv.at[y],
                device_id=y_peer(d), device_id_type=MESH,
            ).start()

    mine = held.at[c, y, z]
    for d in Z_ORDER:
        pltpu.make_async_remote_copy(
            src_ref=mine, dst_ref=mine, send_sem=own_send, recv_sem=z_recv.at[z],
            device_id=z_peer(d), device_id_type=MESH,
        ).start()
    to_y(mine)

    fold = (NOPE + ROPE) ** (-0.5) * math.log2(math.e)
    lane = iota((TOK, 128), 1)
    in_lane, out_lane = iota((128, 128), 0), iota((128, 128), 1)
    turned_tiles = []
    for t in range(HEADS * ROPE // 128):
        tile = qr_ref[:, 128 * t : 128 * t + 128].astype(F32)
        turned_tiles.append((turned(tile, cos_ref[:TOK, :], sin_ref[:TOK, :]) * fold).astype(BF16))
    pick = [
        jnp.where((out_lane < TOK) & (in_lane == ROPE * m + out_lane % ROPE), 1.0, 0.0).astype(BF16)
        for m in range(4)
    ]
    for h in range(HEADS):
        t = h // 2
        plain = qn_ref[:, 128 * t : 128 * t + 128]
        half = lane < NOPE if h % 2 == 0 else lane >= NOPE
        plain = jnp.where(half, plain, jnp.zeros_like(plain))
        lifted = nt_dot(plain, upk_ref[:, 128 * t : 128 * t + 128]) * fold
        q_ref[TOK * h : TOK * h + TOK, :128] = lifted.astype(BF16)
        rotary = jnp.dot(turned_tiles[h // 4], pick[h % 4], preferred_element_type=F32)
        q_ref[TOK * h : TOK * h + TOK, 128:] = rotary.astype(BF16)

    acc_ref[...] = jnp.zeros_like(acc_ref)
    peak_ref[...] = jnp.full_like(peak_ref, NEG_BIG)
    v_ref[LATENT:, :] = jnp.ones((VROWS - LATENT, GROUP), BF16)

    for d in Z_ORDER:
        source = lax.rem(z + d, NZ)
        block = held.at[c, y, source]
        pltpu.make_async_copy(block, block, z_recv.at[source]).wait()
        to_y(block)

    def step(s, _):
        k = lax.rem(s + 1, 3)
        dy = jnp.where(s < 2, 0, jnp.where(k == 0, 1, jnp.where(k == 1, 3, 2)))
        gy = lax.rem(y + dy, NY)
        own = (s == 0) | ((s >= 2) & (s <= 4))
        gc = jnp.where(own, c, 1 - c)
        group = held.at[gc, gy]

        @pl.when(own)
        def _():
            @pl.when(s > 0)
            def _():
                pltpu.make_async_copy(group, group, y_recv.at[gy]).wait()

            pltpu.make_async_remote_copy(
                src_ref=group, dst_ref=group, send_sem=pair_send.at[gy],
                recv_sem=pair_recv.at[gy], device_id=partner, device_id_type=MESH,
            ).start()

        @pl.when(jnp.logical_not(own))
        def _():
            pltpu.make_async_copy(group, group, pair_recv.at[gy]).wait()

        lane32 = iota((32, 128), 1) // ROPE
        for b in range(NZ):
            k_ref[TOK * b : TOK * b + TOK, :128] = held[gc, gy, b, :TOK, :]
            packed = held[gc, gy, b, TOK:, :]
            for j in range(TOK // 32):
                row = TOK * b + 32 * j
                k_ref[row : row + 32, 128:] = jnp.where(lane32 == j, packed, jnp.zeros_like(packed))
        for b in range(GROUP // 128):
            v_ref[:LATENT, 128 * b : 128 * b + 128] = k_ref[128 * b : 128 * b + 128, :128].T

        for n in range(QROWS // CHUNK):
            cols = slice(CHUNK * n, CHUNK * n + CHUNK)
            s_ref[n] = nt_dot(k_ref[...], q_ref[cols, :])
            old = peak_ref[:, cols]
            top = jnp.maximum(old, jnp.max(s_ref[n], axis=0, keepdims=True))
            shrink = jnp.exp2(old - top)
            peak_ref[:, cols] = top
            p_ref[n] = jnp.exp2(s_ref[n] - top).astype(BF16)
            mixed = jnp.dot(v_ref[...], p_ref[n], preferred_element_type=F32)
            acc_ref[:, cols] = acc_ref[:, cols] * shrink + mixed
        return 0

    lax.fori_loop(0, 2 * NY, step, 0)

    lat_t = acc_ref[:LATENT, :] / acc_ref[LATENT : LATENT + 1, :]
    mixed_rows = jnp.concatenate(
        [lat_t[:, 128 * b : 128 * b + 128].T for b in range(QROWS // 128)], axis=0
    ).astype(BF16)
    tiles = []
    for t in range(HEADS // 2):
        up = upv_ref[:, 128 * t : 128 * t + 128]
        even = jnp.dot(mixed_rows[192 * t : 192 * t + 96], up, preferred_element_type=F32)
        odd = jnp.dot(mixed_rows[192 * t + 96 : 192 * t + 192], up, preferred_element_type=F32)
        tiles.append(jnp.where(lane < VDIM, even, odd).astype(BF16))
    attended = jnp.concatenate(tiles, axis=1)
    ow_copy.wait()
    projected = jnp.dot(attended, ow_ref[...], preferred_element_type=F32)
    middle = (res_ref[...].astype(F32) + projected).astype(BF16)
    mid_ref[...] = middle
    wide = middle.astype(F32)
    scale = lax.rsqrt(jnp.mean(wide * wide, axis=-1, keepdims=True) + EPS)
    rows_ref[...] = (wide * scale * fgain_ref[...]).astype(BF16)

    seven = held.at[0, 0, pl.ds(0, NZ - 1)]
    pltpu.make_async_copy(seven, seven, own_send).wait()
    three = held.at[0, pl.ds(0, NY - 1)]
    pltpu.make_async_copy(three, three, fwd_send).wait()
    for g in range(NY):
        group = held.at[c, g]
        pltpu.make_async_copy(group, group, pair_send.at[g]).wait()


def attention(qn, qr, lat, keys, cosine, sine, gain, upk, upv, res, fgain, ow):
    vmem = pl.BlockSpec(memory_space=pltpu.VMEM)
    return pl.pallas_call(
        attention_kernel,
        out_shape=[jax.ShapeDtypeStruct(res.shape, BF16)] * 2,
        in_specs=[vmem] * 11 + [pl.BlockSpec(memory_space=pl.ANY)],
        out_specs=[vmem] * 2,
        scratch_shapes=[
            pltpu.VMEM((2, NY, NZ, 128, 128), BF16),
            pltpu.VMEM((QROWS, 256), BF16),
            pltpu.VMEM((GROUP, 256), BF16),
            pltpu.VMEM((VROWS, GROUP), BF16),
            pltpu.VMEM((QROWS // CHUNK, GROUP, CHUNK), F32),
            pltpu.VMEM((QROWS // CHUNK, GROUP, CHUNK), BF16),
            pltpu.VMEM((VROWS, QROWS), F32),
            pltpu.VMEM((1, QROWS), F32),
            pltpu.VMEM(ow.shape, BF16),
            pltpu.SemaphoreType.DMA,
            pltpu.SemaphoreType.DMA,
            pltpu.SemaphoreType.DMA((NY,)),
            pltpu.SemaphoreType.DMA((NZ,)),
            pltpu.SemaphoreType.DMA((NY,)),
            pltpu.SemaphoreType.DMA((NY,)),
            pltpu.SemaphoreType.DMA,
        ],
        compiler_params=pltpu.CompilerParams(
            collective_id=0, has_side_effects=True, vmem_limit_bytes=56 * 2**20
        ),
    )(qn, qr, lat, keys, cosine, sine, gain, upk, upv, res, fgain, ow)


def local(
    residual,
    query_nope,
    query_rope,
    latent,
    rope_key,
    latent_gain,
    up_key,
    up_value,
    out_weight,
    ffn_gain,
    routes,
    route_weight,
    gate_weight,
    up_weight,
    down_weight,
):
    tokens = residual.shape[1]
    width = residual.shape[2]
    experts = lax.axis_size(SP)
    slots = min(tokens, max(2, 5 * tokens * TOPK // (4 * experts)))
    row, lane = iota((128, 128), 0), iota((128, 128), 1)
    token = jnp.where(row < TOK, row, row - TOK + 32 * (lane // ROPE))
    position = (lax.axis_index(SP) * tokens + token).astype(F32)
    freq = (lane % (ROPE // 2)).astype(F32)
    angle = position * ROPE_BASE ** (-freq * 2.0 / ROPE)
    cosine = jnp.cos(angle)
    sine = jnp.where(lane % ROPE < ROPE // 2, -1.0, 1.0) * jnp.sin(angle)
    keys = jnp.transpose(rope_key[0].reshape(TOK // 32, 32, ROPE), (1, 0, 2)).reshape(32, TOK)
    keys = jnp.pad(keys, ((0, 0), (0, 128 - TOK)))
    middle, normal_rows = attention(
        query_nope[0], query_rope[0], latent[0], keys, cosine, sine,
        latent_gain[None], up_key, up_value, residual[0], ffn_gain[None], out_weight,
    )
    middle_wide = middle.astype(jnp.float32)
    own_picks = lax.dynamic_index_in_dim(routes, lax.axis_index("tp"), 0, keepdims=False)
    own_target = assign(own_picks, slots, experts)
    outgoing = pack_rows(normal_rows, own_target, slots, experts).reshape(1, experts, slots, width)
    arrived = lax.all_to_all(outgoing, SP, split_axis=1, concat_axis=1, tiled=True)

    def partial_rows(piece, start):
        return expert_term(piece.reshape(-1, width), gate_weight[0], up_weight[0], down_weight[0])

    terms = on_gathered_pieces(arrived, "tp", 0, partial_rows, 0)
    mine = sent_and_summed(terms.astype(jnp.bfloat16), "tp", 0)
    returned = lax.all_to_all(
        mine.astype(jnp.bfloat16).reshape(1, experts, slots, width),
        SP,
        split_axis=1,
        concat_axis=1,
        tiled=True,
    )
    picked = returned.reshape(experts * slots, width)[own_target].reshape(tokens, TOPK, width)
    combined = jnp.sum(picked.astype(jnp.float32) * route_weight[0][:, :, None], axis=1)
    return (middle_wide + combined).astype(jnp.bfloat16)[None]


def solution(mesh):
    split = Mesh(mesh.devices.reshape(8, 4, 2, mesh.shape["tp"]), ("sp_0", "sp_1", "sp_2", "tp"))
    in_specs = (
        P("tp", SP, None),
        P("tp", SP, None),
        P("tp", SP, None),
        P("tp", SP, None),
        P("tp", SP, None),
        P(),
        P(),
        P(),
        P(),
        P(),
        P(None, SP, None),
        P("tp", SP, None),
        P(SP, None, "tp"),
        P(SP, None, "tp"),
        P(SP, "tp", None),
    )
    out_specs = P("tp", SP, None)
    return jax.shard_map(local, mesh=split, in_specs=in_specs, out_specs=out_specs, check_vma=False)
```

```python
import math

import jax
import jax.numpy as jnp
from jax import lax
from jax.experimental import pallas as pl
from jax.experimental.pallas import tpu as pltpu
from jax.sharding import Mesh
from jax.sharding import PartitionSpec as P

HEADS = 16
NOPE = 64
ROPE = 32
VDIM = 64
LATENT = 128
TOPK = 2
SP = ("sp_0", "sp_1", "sp_2")

EPS = 1e-06
ROPE_BASE = 10000.0
CLAMP = 7.0
ALPHA = 1.702
NEG_BIG = -1e30
MESH = pl.DeviceIdType.MESH

F32 = jnp.float32
BF16 = jnp.bfloat16
NZ, NY = 8, 4
TOK = 96
GROUP = NZ * TOK
QROWS = HEADS * TOK
CHUNK = 512
VROWS = LATENT + 16
Z_ORDER = (1, 7, 2, 6, 3, 5, 4)


def nt_dot(a, b):
    return lax.dot_general(a, b, (((1,), (1,)), ((), ())), preferred_element_type=F32)


def iota(shape, dim):
    return lax.broadcasted_iota(jnp.int32, shape, dim)


def turned(x, cosine, sine):
    low = iota(x.shape, 1) % ROPE < ROPE // 2
    swapped = jnp.where(low, pltpu.roll(x, 128 - ROPE // 2, 1), pltpu.roll(x, ROPE // 2, 1))
    return x * cosine + swapped * sine


def attention_kernel(
    qn_ref, qr_ref, lat_ref, key_ref, cos_ref, sin_ref, gain_ref, upk_ref, upv_ref,
    res_ref, fgain_ref, ow_hbm,
    mid_ref, rows_ref,
    held, q_ref, k_ref, v_ref, s_ref, p_ref, acc_ref, peak_ref, ow_ref,
    own_send, fwd_send, pair_send, z_recv, y_recv, pair_recv, ow_sem,
):
    z, y, c = (lax.axis_index(name) for name in SP)
    barrier = pltpu.get_barrier_semaphore()

    def z_peer(d):
        return {"sp_0": lax.rem(z + d, NZ)}

    def y_peer(d):
        return {"sp_1": lax.rem(y + d, NY)}

    partner = {"sp_2": 1 - c}
    for d in range(1, NZ):
        pl.semaphore_signal(barrier, inc=1, device_id=z_peer(d), device_id_type=MESH)
    for d in range(1, NY):
        pl.semaphore_signal(barrier, inc=1, device_id=y_peer(d), device_id_type=MESH)
    pl.semaphore_signal(barrier, inc=1, device_id=partner, device_id_type=MESH)
    ow_copy = pltpu.make_async_copy(ow_hbm, ow_ref, ow_sem)
    ow_copy.start()

    wide = lat_ref[...].astype(F32)
    scale = lax.rsqrt(jnp.mean(wide * wide, axis=-1, keepdims=True) + EPS)
    held[c, y, z, :TOK, :] = (wide * scale * gain_ref[...]).astype(BF16)
    held[c, y, z, TOK:, :] = turned(
        key_ref[...].astype(F32), cos_ref[TOK:, :], sin_ref[TOK:, :]
    ).astype(BF16)

    pl.semaphore_wait(barrier, NZ + NY - 1)

    def to_y(block):
        for d in (1, 3, 2):
            pltpu.make_async_remote_copy(
                src_ref=block, dst_ref=block, send_sem=fwd_send, recv_sem=y_recv.at[y],
                device_id=y_peer(d), device_id_type=MESH,
            ).start()

    mine = held.at[c, y, z]
    for d in Z_ORDER:
        pltpu.make_async_remote_copy(
            src_ref=mine, dst_ref=mine, send_sem=own_send, recv_sem=z_recv.at[z],
            device_id=z_peer(d), device_id_type=MESH,
        ).start()
    to_y(mine)

    fold = (NOPE + ROPE) ** (-0.5) * math.log2(math.e)
    lane = iota((TOK, 128), 1)
    in_lane, out_lane = iota((128, 128), 0), iota((128, 128), 1)
    turned_tiles = []
    for t in range(HEADS * ROPE // 128):
        tile = qr_ref[:, 128 * t : 128 * t + 128].astype(F32)
        turned_tiles.append((turned(tile, cos_ref[:TOK, :], sin_ref[:TOK, :]) * fold).astype(BF16))
    pick = [
        jnp.where((out_lane < TOK) & (in_lane == ROPE * m + out_lane % ROPE), 1.0, 0.0).astype(BF16)
        for m in range(4)
    ]
    for h in range(HEADS):
        t = h // 2
        plain = qn_ref[:, 128 * t : 128 * t + 128]
        half = lane < NOPE if h % 2 == 0 else lane >= NOPE
        plain = jnp.where(half, plain, jnp.zeros_like(plain))
        lifted = nt_dot(plain, upk_ref[:, 128 * t : 128 * t + 128]) * fold
        q_ref[TOK * h : TOK * h + TOK, :128] = lifted.astype(BF16)
        rotary = jnp.dot(turned_tiles[h // 4], pick[h % 4], preferred_element_type=F32)
        q_ref[TOK * h : TOK * h + TOK, 128:] = rotary.astype(BF16)

    acc_ref[...] = jnp.zeros_like(acc_ref)
    peak_ref[...] = jnp.full_like(peak_ref, NEG_BIG)
    v_ref[LATENT:, :] = jnp.ones((VROWS - LATENT, GROUP), BF16)

    for d in Z_ORDER:
        source = lax.rem(z + d, NZ)
        block = held.at[c, y, source]
        pltpu.make_async_copy(block, block, z_recv.at[source]).wait()
        to_y(block)

    def step(s, _):
        k = lax.rem(s + 1, 3)
        dy = jnp.where(s < 2, 0, jnp.where(k == 0, 1, jnp.where(k == 1, 3, 2)))
        gy = lax.rem(y + dy, NY)
        own = (s == 0) | ((s >= 2) & (s <= 4))
        gc = jnp.where(own, c, 1 - c)
        group = held.at[gc, gy]

        @pl.when(own)
        def _():
            @pl.when(s > 0)
            def _():
                pltpu.make_async_copy(group, group, y_recv.at[gy]).wait()

            pltpu.make_async_remote_copy(
                src_ref=group, dst_ref=group, send_sem=pair_send.at[gy],
                recv_sem=pair_recv.at[gy], device_id=partner, device_id_type=MESH,
            ).start()

        @pl.when(jnp.logical_not(own))
        def _():
            pltpu.make_async_copy(group, group, pair_recv.at[gy]).wait()

        lane32 = iota((32, 128), 1) // ROPE
        for b in range(NZ):
            k_ref[TOK * b : TOK * b + TOK, :128] = held[gc, gy, b, :TOK, :]
            packed = held[gc, gy, b, TOK:, :]
            for j in range(TOK // 32):
                row = TOK * b + 32 * j
                k_ref[row : row + 32, 128:] = jnp.where(lane32 == j, packed, jnp.zeros_like(packed))
        for b in range(GROUP // 128):
            v_ref[:LATENT, 128 * b : 128 * b + 128] = k_ref[128 * b : 128 * b + 128, :128].T

        for n in range(QROWS // CHUNK):
            cols = slice(CHUNK * n, CHUNK * n + CHUNK)
            s_ref[n] = nt_dot(k_ref[...], q_ref[cols, :])
            old = peak_ref[:, cols]
            top = jnp.maximum(old, jnp.max(s_ref[n], axis=0, keepdims=True))
            shrink = jnp.exp2(old - top)
            peak_ref[:, cols] = top
            p_ref[n] = jnp.exp2(s_ref[n] - top).astype(BF16)
            mixed = jnp.dot(v_ref[...], p_ref[n], preferred_element_type=F32)
            acc_ref[:, cols] = acc_ref[:, cols] * shrink + mixed
        return 0

    lax.fori_loop(0, 2 * NY, step, 0)

    lat_t = acc_ref[:LATENT, :] / acc_ref[LATENT : LATENT + 1, :]
    mixed_rows = jnp.concatenate(
        [lat_t[:, 128 * b : 128 * b + 128].T for b in range(QROWS // 128)], axis=0
    ).astype(BF16)
    tiles = []
    for t in range(HEADS // 2):
        up = upv_ref[:, 128 * t : 128 * t + 128]
        even = jnp.dot(mixed_rows[192 * t : 192 * t + 96], up, preferred_element_type=F32)
        odd = jnp.dot(mixed_rows[192 * t + 96 : 192 * t + 192], up, preferred_element_type=F32)
        tiles.append(jnp.where(lane < VDIM, even, odd).astype(BF16))
    attended = jnp.concatenate(tiles, axis=1)
    ow_copy.wait()
    projected = jnp.dot(attended, ow_ref[...], preferred_element_type=F32)
    middle = (res_ref[...].astype(F32) + projected).astype(BF16)
    mid_ref[...] = middle
    wide = middle.astype(F32)
    scale = lax.rsqrt(jnp.mean(wide * wide, axis=-1, keepdims=True) + EPS)
    rows_ref[...] = (wide * scale * fgain_ref[...]).astype(BF16)

    seven = held.at[0, 0, pl.ds(0, NZ - 1)]
    pltpu.make_async_copy(seven, seven, own_send).wait()
    three = held.at[0, pl.ds(0, NY - 1)]
    pltpu.make_async_copy(three, three, fwd_send).wait()
    for g in range(NY):
        group = held.at[c, g]
        pltpu.make_async_copy(group, group, pair_send.at[g]).wait()


def attention(qn, qr, lat, keys, cosine, sine, gain, upk, upv, res, fgain, ow):
    vmem = pl.BlockSpec(memory_space=pltpu.VMEM)
    return pl.pallas_call(
        attention_kernel,
        out_shape=[jax.ShapeDtypeStruct(res.shape, BF16)] * 2,
        in_specs=[vmem] * 11 + [pl.BlockSpec(memory_space=pl.ANY)],
        out_specs=[vmem] * 2,
        scratch_shapes=[
            pltpu.VMEM((2, NY, NZ, 128, 128), BF16),
            pltpu.VMEM((QROWS, 256), BF16),
            pltpu.VMEM((GROUP, 256), BF16),
            pltpu.VMEM((VROWS, GROUP), BF16),
            pltpu.VMEM((QROWS // CHUNK, GROUP, CHUNK), F32),
            pltpu.VMEM((QROWS // CHUNK, GROUP, CHUNK), BF16),
            pltpu.VMEM((VROWS, QROWS), F32),
            pltpu.VMEM((1, QROWS), F32),
            pltpu.VMEM(ow.shape, BF16),
            pltpu.SemaphoreType.DMA,
            pltpu.SemaphoreType.DMA,
            pltpu.SemaphoreType.DMA((NY,)),
            pltpu.SemaphoreType.DMA((NZ,)),
            pltpu.SemaphoreType.DMA((NY,)),
            pltpu.SemaphoreType.DMA((NY,)),
            pltpu.SemaphoreType.DMA,
        ],
        compiler_params=pltpu.CompilerParams(
            collective_id=0, has_side_effects=True, vmem_limit_bytes=56 * 2**20
        ),
    )(qn, qr, lat, keys, cosine, sine, gain, upk, upv, res, fgain, ow)


CHUNK_ROWS = 3 * 16
Z_ROWS = 8 * CHUNK_ROWS
ALL_ROWS = 64 * CHUNK_ROWS
WIDTH = 2048
STAGES = 5


def mixed_tiles(x, outer, inner):
    return jnp.concatenate(
        [
            jnp.concatenate(
                [x[16 * a : 16 * a + 16, 128 * j : 128 * j + 128] for a in range(outer)], axis=1
            )
            for j in range(inner)
        ],
        axis=0,
    )


def side_by_side(x):
    return jnp.concatenate([x[256 * a : 256 * a + 256] for a in range(x.shape[0] // 256)], axis=1)


def stacked(x):
    return jnp.concatenate([x[:, 128 * a : 128 * a + 128] for a in range(x.shape[1] // 128)], axis=0)


def swap_matrix():
    row, col = iota((256, 256), 0), iota((256, 256), 1)
    return jnp.where(col == (row % 16) * 16 + row // 16, 1.0, 0.0).astype(BF16)


def to_chunks(rows, swap):
    mixed = mixed_tiles(rows, rows.shape[0] // 16, 16)
    return stacked(jnp.dot(swap, mixed, preferred_element_type=F32).astype(BF16))


def from_chunks(chunks, swap):
    mixed = jnp.dot(swap, side_by_side(chunks), preferred_element_type=F32).astype(BF16)
    return mixed_tiles(mixed, 16, chunks.shape[0] // 256)


def experts_kernel(
    rows_ref, mid_ref, routes_ref, rw_ref, gate_hbm, up_hbm, down_hbm,
    out_ref,
    packed, rows_in, made, part, sums, back, home, swap_ref, gate_ref, up_ref, down_ref,
    w_sem, a_send, b_send, f_send, p_send, q_send, e_send,
    a_recv, b_recv, f_recv, p_recv, q_recv, e_recv,
):
    z, y, c = (lax.axis_index(name) for name in SP)
    x = lax.axis_index("tp")
    me = (z * NY + y) * 2 + c
    after, before, across = (lax.rem(x + d, 4) for d in (1, 3, 2))
    barrier = pltpu.get_barrier_semaphore()
    copies = [
        pltpu.make_async_copy(gate_hbm.at[0], gate_ref, w_sem.at[0]),
        pltpu.make_async_copy(up_hbm.at[0], up_ref, w_sem.at[1]),
        pltpu.make_async_copy(down_hbm.at[0], down_ref, w_sem.at[2]),
    ]

    def peer(step, k):
        dz = jnp.where(lax.rem(step, 2) == 1, (step + 1) // 2, NZ - step // 2)
        pz, py, pc = lax.rem(z + dz, NZ), lax.rem(y + k // 2, NY), lax.rem(c + k, 2)
        return {"sp_0": pz, "sp_1": py, "sp_2": pc}, (pz * NY + py) * 2 + pc

    def group_of(step):
        dz = jnp.where(lax.rem(step, 2) == 1, (step + 1) // 2, NZ - step // 2)
        return lax.rem(z + NZ - lax.rem(dz, NZ), NZ)

    def greet(n, _):
        pl.semaphore_signal(barrier, inc=1, device_id=peer(n // 8, lax.rem(n, 8))[0], device_id_type=MESH)
        return 0

    lax.fori_loop(1, 64, greet, 0)
    for other in (after, before):
        pl.semaphore_signal(barrier, inc=1, device_id={"tp": other}, device_id_type=MESH)
    for copy in copies:
        copy.start()

    swap_ref[...] = swap_matrix()
    swap = swap_ref[...]
    picks = routes_ref[x].astype(F32)
    down_i, right_i = iota((TOK, TOK), 0), iota((TOK, TOK), 1)
    col = [picks[:, k : k + 1] for k in range(TOPK)]
    row = [
        jnp.sum(jnp.where(down_i == right_i, col[k], 0.0), axis=0, keepdims=True)
        for k in range(TOPK)
    ]
    earlier_r = jnp.where(down_i < right_i, 1.0, 0.0)
    earlier_c = jnp.where(right_i < down_i, 1.0, 0.0)

    def same(a, b):
        return jnp.where(a == b, 1.0, 0.0)

    rank_row = [
        jnp.sum(same(col[0], row[0]) * earlier_r, axis=0, keepdims=True),
        jnp.sum(same(col[0], row[1]) + same(col[1], row[1]) * earlier_r, axis=0, keepdims=True),
    ]
    rank_col = [
        jnp.sum(same(row[0], col[0]) * earlier_c, axis=1, keepdims=True),
        jnp.sum(same(row[0], col[1]) + same(row[1], col[1]) * earlier_c, axis=1, keepdims=True),
    ]
    slot_d = iota((2 * TOK, TOK), 0).astype(F32)
    spread = sum(same(slot_d, 3.0 * row[k] + rank_row[k]) for k in range(TOPK)).astype(BF16)
    sent = jnp.dot(spread, rows_ref[...], preferred_element_type=F32).astype(BF16)
    packed[...] = to_chunks(sent, swap)

    pl.semaphore_wait(barrier, 65)

    def block(index):
        return pl.ds(pl.multiple_of(index * CHUNK_ROWS, CHUNK_ROWS), CHUNK_ROWS)

    def group(g, half=None):
        if half is None:
            return pl.ds(pl.multiple_of(g * Z_ROWS, Z_ROWS), Z_ROWS)
        return pl.ds(pl.multiple_of(g * Z_ROWS + half * (Z_ROWS // 2), Z_ROWS // 2), Z_ROWS // 2)

    own_copy = pltpu.make_async_copy(packed.at[block(me)], rows_in.at[x, block(me)], a_recv.at[z])
    own_copy.start()

    def dispatch(n, _):
        where, index = peer(n // 8, lax.rem(n, 8))
        pltpu.make_async_remote_copy(
            src_ref=packed.at[block(index)], dst_ref=rows_in.at[x, block(me)],
            send_sem=a_send, recv_sem=a_recv.at[z], device_id=where, device_id_type=MESH,
        ).start()
        return 0

    lax.fori_loop(1, 64, dispatch, 0)
    for copy in copies:
        copy.wait()

    def send(src, dst, ssem, rsem, other):
        pltpu.make_async_remote_copy(
            src_ref=src, dst_ref=dst, send_sem=ssem, recv_sem=rsem,
            device_id={"tp": other}, device_id_type=MESH,
        ).start()

    def await_(ref, sem):
        pltpu.make_async_copy(ref, ref, sem).wait()

    sides = ((0, after), (1, before))

    def turn(t, _):
        @pl.when(t < NZ)
        def _():
            g = group_of(t)
            ref = rows_in.at[x, group(g)]
            await_(ref, a_recv.at[g])
            for side, other in sides:
                send(ref, ref, b_send, b_recv.at[side, g], other)

        @pl.when((t >= 1) & (t < NZ + 1))
        def _():
            g = group_of(t - 1)
            for side, other in sides:
                origin = before if side == 0 else after
                await_(rows_in.at[origin, group(g)], b_recv.at[side, g])
                ref = rows_in.at[origin, group(g, side)]
                send(ref, ref, f_send, f_recv.at[side, g], other)

        @pl.when((t >= 2) & (t < NZ + 2))
        def _():
            g = group_of(t - 2)
            for side, _other in sides:
                await_(rows_in.at[across, group(g, side)], f_recv.at[side, g])
            chunks = jnp.concatenate([rows_in[s, group(g)] for s in range(4)], axis=0)
            rows = from_chunks(chunks, swap_ref[...])
            gate = jnp.minimum(jnp.dot(rows, gate_ref[...], preferred_element_type=F32), CLAMP)
            lift = jnp.clip(jnp.dot(rows, up_ref[...], preferred_element_type=F32), -CLAMP, CLAMP)
            active = (gate * jax.nn.sigmoid(ALPHA * gate) * (lift + 1.0)).astype(BF16)
            result = jnp.dot(active, down_ref[...], preferred_element_type=F32).astype(BF16)
            chunks = to_chunks(result, swap_ref[...])
            for s in range(4):
                made[s, group(g)] = chunks[Z_ROWS * s : Z_ROWS * s + Z_ROWS]
            for side, other in sides:
                send(made.at[across, group(g, side)], part.at[side, g], p_send, p_recv.at[side, g], other)

        @pl.when((t >= 3) & (t < NZ + 3))
        def _():
            g = group_of(t - 3)
            for side, other in sides:
                await_(part.at[side, g], p_recv.at[side, g])
                add = made[other, group(g, side)].astype(F32) + part[side, g].astype(F32)
                made[other, group(g, side)] = add.astype(BF16)
                send(made.at[other, group(g)], sums.at[side, g], q_send, q_recv.at[side, g], other)

        @pl.when(t >= 4)
        def _():
            g = group_of(t - 4)
            for side, _other in sides:
                await_(sums.at[side, g], q_recv.at[side, g])
            total = made[x, group(g)].astype(F32) + sums[0, g].astype(F32) + sums[1, g].astype(F32)
            back[group(g)] = total.astype(BF16)

            def give(k, _):
                py, pc = lax.rem(y + k // 2, NY), lax.rem(c + k, 2)
                index = (g * NY + py) * 2 + pc
                is_me = index == me

                @pl.when(is_me)
                def _():
                    pltpu.make_async_copy(
                        back.at[block(me)], home.at[block(me)], e_recv.at[z]
                    ).start()

                @pl.when(jnp.logical_not(is_me))
                def _():
                    pltpu.make_async_remote_copy(
                        src_ref=back.at[block(index)], dst_ref=home.at[block(me)],
                        send_sem=e_send, recv_sem=e_recv.at[z],
                        device_id={"sp_0": g, "sp_1": py, "sp_2": pc}, device_id_type=MESH,
                    ).start()

                return 0

            lax.fori_loop(0, 8, give, 0)

        return 0

    lax.fori_loop(0, NZ + STAGES - 1, turn, 0)

    slot_c = iota((TOK, 2 * TOK), 1).astype(F32)
    weight = sum(
        same(slot_c, 3.0 * col[k] + rank_col[k]) * rw_ref[:, k : k + 1] for k in range(TOPK)
    )
    high = weight.astype(BF16)
    low = (weight - high.astype(F32)).astype(BF16)
    for g in range(NZ):
        await_(home.at[group(g)], e_recv.at[g])
    results = from_chunks(home[...], swap_ref[...])
    combined = jnp.dot(high, results, preferred_element_type=F32) + jnp.dot(
        low, results, preferred_element_type=F32
    )
    out_ref[...] = (mid_ref[...].astype(F32) + combined).astype(BF16)

    most = pl.ds(0, ALL_ROWS - CHUNK_ROWS)
    await_(packed.at[most], a_send)
    await_(back.at[most], e_send)
    await_(rows_in.at[pl.ds(0, 2)], b_send)
    await_(rows_in.at[0], f_send)
    await_(made.at[0], p_send)
    await_(made.at[pl.ds(0, 2)], q_send)


def run_experts(rows, middle, routes, route_weight, gate_weight, up_weight, down_weight):
    vmem = pl.BlockSpec(memory_space=pltpu.VMEM)
    anywhere = pl.BlockSpec(memory_space=pl.ANY)
    dma = pltpu.SemaphoreType.DMA
    return pl.pallas_call(
        experts_kernel,
        out_shape=jax.ShapeDtypeStruct(middle.shape, BF16),
        in_specs=[vmem] * 4 + [anywhere] * 3,
        out_specs=vmem,
        scratch_shapes=[
            pltpu.VMEM((ALL_ROWS, 128), BF16),
            pltpu.VMEM((4, ALL_ROWS, 128), BF16),
            pltpu.VMEM((4, ALL_ROWS, 128), BF16),
            pltpu.VMEM((2, NZ, Z_ROWS // 2, 128), BF16),
            pltpu.VMEM((2, NZ, Z_ROWS, 128), BF16),
            pltpu.VMEM((ALL_ROWS, 128), BF16),
            pltpu.VMEM((ALL_ROWS, 128), BF16),
            pltpu.VMEM((256, 256), BF16),
            pltpu.VMEM(gate_weight.shape[1:], BF16),
            pltpu.VMEM(up_weight.shape[1:], BF16),
            pltpu.VMEM(down_weight.shape[1:], BF16),
            dma((3,)), dma, dma, dma, dma, dma, dma,
            dma((NZ,)), dma((2, NZ)), dma((2, NZ)), dma((2, NZ)), dma((2, NZ)), dma((NZ,)),
        ],
        compiler_params=pltpu.CompilerParams(
            collective_id=1, has_side_effects=True, vmem_limit_bytes=56 * 2**20
        ),
    )(rows, middle, routes, route_weight, gate_weight, up_weight, down_weight)


def local(
    residual,
    query_nope,
    query_rope,
    latent,
    rope_key,
    latent_gain,
    up_key,
    up_value,
    out_weight,
    ffn_gain,
    routes,
    route_weight,
    gate_weight,
    up_weight,
    down_weight,
):
    tokens = residual.shape[1]
    row, lane = iota((128, 128), 0), iota((128, 128), 1)
    token = jnp.where(row < TOK, row, row - TOK + 32 * (lane // ROPE))
    position = (lax.axis_index(SP) * tokens + token).astype(F32)
    freq = (lane % (ROPE // 2)).astype(F32)
    angle = position * ROPE_BASE ** (-freq * 2.0 / ROPE)
    cosine = jnp.cos(angle)
    sine = jnp.where(lane % ROPE < ROPE // 2, -1.0, 1.0) * jnp.sin(angle)
    keys = jnp.transpose(rope_key[0].reshape(TOK // 32, 32, ROPE), (1, 0, 2)).reshape(32, TOK)
    keys = jnp.pad(keys, ((0, 0), (0, 128 - TOK)))
    middle, normal_rows = attention(
        query_nope[0], query_rope[0], latent[0], keys, cosine, sine,
        latent_gain[None], up_key, up_value, residual[0], ffn_gain[None], out_weight,
    )
    updated = run_experts(
        normal_rows, middle, routes, route_weight[0], gate_weight, up_weight, down_weight
    )
    return updated[None]


def solution(mesh):
    split = Mesh(mesh.devices.reshape(8, 4, 2, mesh.shape["tp"]), ("sp_0", "sp_1", "sp_2", "tp"))
    in_specs = (
        P("tp", SP, None),
        P("tp", SP, None),
        P("tp", SP, None),
        P("tp", SP, None),
        P("tp", SP, None),
        P(),
        P(),
        P(),
        P(),
        P(),
        P(None, SP, None),
        P("tp", SP, None),
        P(SP, None, "tp"),
        P(SP, None, "tp"),
        P(SP, "tp", None),
    )
    out_specs = P("tp", SP, None)
    return jax.shard_map(local, mesh=split, in_specs=in_specs, out_specs=out_specs, check_vma=False)
```

```python
import math

import jax
import jax.numpy as jnp
import numpy as np
from jax import lax
from jax.experimental import pallas as pl
from jax.experimental.pallas import tpu as pltpu
from jax.sharding import Mesh
from jax.sharding import PartitionSpec as P

HEADS = 16
NOPE = 64
ROPE = 32
VDIM = 64
LATENT = 128
TOPK = 2
SP = ("sp_0", "sp_1", "sp_2")

EPS = 1e-06
ROPE_BASE = 10000.0
CLAMP = 7.0
ALPHA = 1.702
NEG_BIG = -1e30
MESH = pl.DeviceIdType.MESH

F32 = jnp.float32
BF16 = jnp.bfloat16
NZ, NY = 8, 4
TOK = 96
GROUP = NZ * TOK
QROWS = HEADS * TOK
CHUNK = 512
VROWS = LATENT + 16
Z_ORDER = (1, 7, 2, 6, 3, 5, 4)
ROW_ORDER = (0, 1, 2, 6, 5, 4, 3, 7)
FF_BLOCK = 256
ACT_ROWS = 32


def nt_dot(a, b):
    return lax.dot_general(a, b, (((1,), (1,)), ((), ())), preferred_element_type=F32)


def iota(shape, dim):
    return lax.broadcasted_iota(jnp.int32, shape, dim)


def turned(x, cosine, sine):
    low = iota(x.shape, 1) % ROPE < ROPE // 2
    swapped = jnp.where(low, pltpu.roll(x, 128 - ROPE // 2, 1), pltpu.roll(x, ROPE // 2, 1))
    return x * cosine + swapped * sine


CHUNK_ROWS = 3 * 16
Z_ROWS = 8 * CHUNK_ROWS
ALL_ROWS = 64 * CHUNK_ROWS
WIDTH = 2048
STAGES = 4


def mixed_tiles(x, outer, inner):
    return jnp.concatenate(
        [
            jnp.concatenate(
                [x[16 * a : 16 * a + 16, 128 * j : 128 * j + 128] for a in range(outer)], axis=1
            )
            for j in range(inner)
        ],
        axis=0,
    )


def side_by_side(x):
    return jnp.concatenate([x[256 * a : 256 * a + 256] for a in range(x.shape[0] // 256)], axis=1)


def stacked(x):
    return jnp.concatenate([x[:, 128 * a : 128 * a + 128] for a in range(x.shape[1] // 128)], axis=0)


def swap_matrix():
    row, col = iota((256, 256), 0), iota((256, 256), 1)
    return jnp.where(col == (row % 16) * 16 + row // 16, 1.0, 0.0).astype(BF16)


def to_chunks(rows, swap):
    mixed = mixed_tiles(rows, rows.shape[0] // 16, 16)
    return stacked(jnp.dot(swap, mixed, preferred_element_type=F32).astype(BF16))


def from_chunks(chunks, swap):
    mixed = jnp.dot(swap, side_by_side(chunks), preferred_element_type=F32).astype(BF16)
    return mixed_tiles(mixed, 16, chunks.shape[0] // 256)


def layer_kernel(
    gain_ref, fgain_ref, inv_ref, routes_ref, rw_ref,
    res_hbm, qn_hbm, qr_hbm, lat_hbm, key_hbm, upk_hbm, upv_hbm, ow_hbm, gate_hbm, up_hbm, down_hbm,
    out_ref,
    res_ref, qn_ref, qr_ref, lat_ref, key_ref, upk_ref, upv_ref, ow_ref, gate_ref, up_ref, down_ref,
    held, q_ref, k_ref, v_ref, s_ref, p_ref, acc_ref, peak_ref,
    mid_ref, packed, rows_in, act_out, act_in, back, home, swap_ref, mix_ref,
    in_sem, own_send, fwd_send, pair_send, d_send, h_send, a_send, b_send, f_send, g_send, e_send,
    z_recv, y_recv, pair_recv, d_recv, h_recv, a_recv, b_recv, f_recv, g_recv, e_recv,
):
    z, y, c = (lax.axis_index(name) for name in SP)
    x = lax.axis_index("tp")
    me = (z * NY + y) * 2 + c
    after, before, across = (lax.rem(x + d, 4) for d in (1, 3, 2))
    sides = ((0, after, before), (1, before, after))
    barrier = pltpu.get_barrier_semaphore()

    def distance(step):
        dz = 0
        for n, d in enumerate(ROW_ORDER):
            dz = dz + jnp.where(step == n, d, 0)
        return dz

    def peer(step, k):
        pz = lax.rem(z + distance(step), NZ)
        py, pc = lax.rem(y + k // 2, NY), lax.rem(c + k, 2)
        return {"sp_0": pz, "sp_1": py, "sp_2": pc}, (pz * NY + py) * 2 + pc

    def group_of(step):
        return lax.rem(z + NZ - distance(step), NZ)

    def greet(n, _):
        where = peer(n // 8, lax.rem(n, 8))[0]
        pl.semaphore_signal(barrier, inc=1, device_id=where, device_id_type=MESH)
        return 0

    lax.fori_loop(1, 64, greet, 0)
    for other in (after, before, across):
        pl.semaphore_signal(barrier, inc=1, device_id={"tp": other}, device_id_type=MESH)

    loads = {}
    for n, (name, src, dst) in enumerate((
        ("lat", lat_hbm.at[0], lat_ref),
        ("key", key_hbm.at[0], key_ref),
        ("down", down_hbm.at[0], down_ref.at[x]),
        ("qn", qn_hbm.at[0], qn_ref),
        ("qr", qr_hbm.at[0], qr_ref),
        ("upk", upk_hbm, upk_ref),
        ("upv", upv_hbm, upv_ref),
        ("res", res_hbm.at[0], res_ref),
        ("ow", ow_hbm, ow_ref),
        ("gate", gate_hbm.at[0], gate_ref),
        ("up", up_hbm.at[0], up_ref),
    )):
        loads[name] = pltpu.make_async_copy(src, dst, in_sem.at[n])
        loads[name].start()

    def await_(ref, sem):
        pltpu.make_async_copy(ref, ref, sem).wait()

    def send(src, dst, ssem, rsem, where):
        pltpu.make_async_remote_copy(
            src_ref=src, dst_ref=dst, send_sem=ssem, recv_sem=rsem,
            device_id=where, device_id_type=MESH,
        ).start()

    row, lane = iota((128, 128), 0), iota((128, 128), 1)
    token = jnp.where(row < TOK, row, row - TOK + 32 * (lane // ROPE))
    angle = (me * TOK + token).astype(F32) * inv_ref[...]
    cosine = jnp.cos(angle)
    sine = jnp.where(lane % ROPE < ROPE // 2, -1.0, 1.0) * jnp.sin(angle)

    loads["lat"].wait()
    wide = lat_ref[...].astype(F32)
    scale = lax.rsqrt(jnp.mean(wide * wide, axis=-1, keepdims=True) + EPS)
    held[c, y, z, :TOK, :] = (wide * scale * gain_ref[...]).astype(BF16)
    loads["key"].wait()
    raw = key_ref[...]
    keys = jnp.zeros((32, 128), F32)
    for j in range(TOK // 32):
        chosen = jnp.where(iota((32, TOK), 1) == 32 * j + iota((32, TOK), 0), 1.0, 0.0)
        blank = [jnp.zeros((32, TOK), BF16)] * 4
        blank[j] = raw
        keys = keys + nt_dot(chosen.astype(BF16), jnp.concatenate(blank, axis=0))
    held[c, y, z, TOK:, :] = turned(keys, cosine[TOK:], sine[TOK:]).astype(BF16)

    pl.semaphore_wait(barrier, 66)

    def to_y(block):
        for d in (1, 3, 2):
            send(block, block, fwd_send, y_recv.at[y], {"sp_1": lax.rem(y + d, NY)})

    mine = held.at[c, y, z]
    for d in Z_ORDER:
        send(mine, mine, own_send, z_recv.at[z], {"sp_0": lax.rem(z + d, NZ)})
    to_y(mine)

    loads["down"].wait()
    half_ff = FF_BLOCK // 2
    for side, other, _origin in sides:
        for h in (side, 1 - side):
            piece = down_ref.at[x, pl.ds(half_ff * h, half_ff)]
            send(piece, piece, d_send, d_recv.at[side, h], {"tp": other})

    fold = (NOPE + ROPE) ** (-0.5) * math.log2(math.e)
    lane = iota((TOK, 128), 1)
    in_lane, out_lane = iota((128, 128), 0), iota((128, 128), 1)
    for name in ("qn", "qr", "upk"):
        loads[name].wait()
    turned_tiles = []
    for t in range(HEADS * ROPE // 128):
        tile = qr_ref[:, 128 * t : 128 * t + 128].astype(F32)
        turned_tiles.append((turned(tile, cosine[:TOK], sine[:TOK]) * fold).astype(BF16))
    pick = [
        jnp.where((out_lane < TOK) & (in_lane == ROPE * m + out_lane % ROPE), 1.0, 0.0).astype(BF16)
        for m in range(4)
    ]
    for h in range(HEADS):
        t = h // 2
        plain = qn_ref[:, 128 * t : 128 * t + 128]
        half = lane < NOPE if h % 2 == 0 else lane >= NOPE
        plain = jnp.where(half, plain, jnp.zeros_like(plain))
        lifted = nt_dot(plain, upk_ref[:, 128 * t : 128 * t + 128]) * fold
        q_ref[TOK * h : TOK * h + TOK, :128] = lifted.astype(BF16)
        rotary = jnp.dot(turned_tiles[h // 4], pick[h % 4], preferred_element_type=F32)
        q_ref[TOK * h : TOK * h + TOK, 128:] = rotary.astype(BF16)

    acc_ref[...] = jnp.zeros_like(acc_ref)
    peak_ref[...] = jnp.full_like(peak_ref, NEG_BIG)
    v_ref[LATENT:, :] = jnp.ones((VROWS - LATENT, GROUP), BF16)
    swap_ref[...] = swap_matrix()

    for d in Z_ORDER:
        source = lax.rem(z + d, NZ)
        block = held.at[c, y, source]
        await_(block, z_recv.at[source])
        to_y(block)

    def step(s, _):
        k = lax.rem(s + 1, 3)
        dy = jnp.where(s < 2, 0, jnp.where(k == 0, 1, jnp.where(k == 1, 3, 2)))
        gy = lax.rem(y + dy, NY)
        own = (s == 0) | ((s >= 2) & (s <= 4))
        gc = jnp.where(own, c, 1 - c)
        group = held.at[gc, gy]

        @pl.when(own)
        def _():
            @pl.when(s > 0)
            def _():
                await_(group, y_recv.at[gy])

            send(group, group, pair_send.at[gy], pair_recv.at[gy], {"sp_2": 1 - c})

        @pl.when(jnp.logical_not(own))
        def _():
            await_(group, pair_recv.at[gy])

        @pl.when(s == 3)
        def _():
            for side, other, origin in sides:
                piece = down_ref.at[origin, pl.ds(half_ff * side, half_ff)]
                await_(piece, d_recv.at[side, side])
                send(piece, piece, h_send, h_recv.at[side], {"tp": other})

        lane32 = iota((32, 128), 1) // ROPE
        for b in range(NZ):
            k_ref[TOK * b : TOK * b + TOK, :128] = held[gc, gy, b, :TOK, :]
            packed_keys = held[gc, gy, b, TOK:, :]
            for j in range(TOK // 32):
                first = TOK * b + 32 * j
                k_ref[first : first + 32, 128:] = jnp.where(
                    lane32 == j, packed_keys, jnp.zeros_like(packed_keys)
                )
        for b in range(GROUP // 128):
            v_ref[:LATENT, 128 * b : 128 * b + 128] = k_ref[128 * b : 128 * b + 128, :128].T

        for n in range(QROWS // CHUNK):
            cols = slice(CHUNK * n, CHUNK * n + CHUNK)
            s_ref[n] = nt_dot(k_ref[...], q_ref[cols, :])
            old = peak_ref[:, cols]
            top = jnp.maximum(old, jnp.max(s_ref[n], axis=0, keepdims=True))
            shrink = jnp.exp2(old - top)
            peak_ref[:, cols] = top
            p_ref[n] = jnp.exp2(s_ref[n] - top).astype(BF16)
            mixed = jnp.dot(v_ref[...], p_ref[n], preferred_element_type=F32)
            acc_ref[:, cols] = acc_ref[:, cols] * shrink + mixed
        return 0

    lax.fori_loop(0, 2 * NY, step, 0)

    lat_t = acc_ref[:LATENT, :] / acc_ref[LATENT : LATENT + 1, :]
    mixed_rows = jnp.concatenate(
        [lat_t[:, 128 * b : 128 * b + 128].T for b in range(QROWS // 128)], axis=0
    ).astype(BF16)
    tiles = []
    loads["upv"].wait()
    for t in range(HEADS // 2):
        up = upv_ref[:, 128 * t : 128 * t + 128]
        even = jnp.dot(mixed_rows[192 * t : 192 * t + 96], up, preferred_element_type=F32)
        odd = jnp.dot(mixed_rows[192 * t + 96 : 192 * t + 192], up, preferred_element_type=F32)
        tiles.append(jnp.where(lane < VDIM, even, odd).astype(BF16))
    attended = jnp.concatenate(tiles, axis=1)
    loads["ow"].wait()
    loads["res"].wait()
    projected = jnp.dot(attended, ow_ref[...], preferred_element_type=F32)
    middle = (res_ref[...].astype(F32) + projected).astype(BF16)
    mid_ref[...] = middle
    wide = middle.astype(F32)
    scale = lax.rsqrt(jnp.mean(wide * wide, axis=-1, keepdims=True) + EPS)
    normal_rows = (wide * scale * fgain_ref[...]).astype(BF16)

    picks = routes_ref[x].astype(F32)
    down_i, right_i = iota((TOK, TOK), 0), iota((TOK, TOK), 1)

    def as_column(line):
        return jnp.sum(jnp.where(down_i == right_i, line, 0.0), axis=1, keepdims=True)

    row = [picks[k : k + 1, :] for k in range(TOPK)]
    col = [as_column(line) for line in row]
    earlier_r = jnp.where(down_i < right_i, 1.0, 0.0)
    earlier_c = jnp.where(right_i < down_i, 1.0, 0.0)

    def same(a, b):
        return jnp.where(a == b, 1.0, 0.0)

    rank_row = [
        jnp.sum(same(col[0], row[0]) * earlier_r, axis=0, keepdims=True),
        jnp.sum(same(col[0], row[1]) + same(col[1], row[1]) * earlier_r, axis=0, keepdims=True),
    ]
    rank_col = [
        jnp.sum(same(row[0], col[0]) * earlier_c, axis=1, keepdims=True),
        jnp.sum(same(row[0], col[1]) + same(row[1], col[1]) * earlier_c, axis=1, keepdims=True),
    ]
    slot_d = iota((2 * TOK, TOK), 0).astype(F32)
    spread = sum(same(slot_d, 3.0 * row[k] + rank_row[k]) for k in range(TOPK)).astype(BF16)
    sent = jnp.dot(spread, normal_rows, preferred_element_type=F32).astype(BF16)
    packed[...] = to_chunks(sent, swap_ref[...])
    slot_c = iota((TOK, 2 * TOK), 1).astype(F32)
    weight = sum(
        same(slot_c, 3.0 * col[k] + rank_col[k]) * as_column(rw_ref[k : k + 1, :])
        for k in range(TOPK)
    )
    high = weight.astype(BF16)
    mix_ref[0] = high
    mix_ref[1] = (weight - high.astype(F32)).astype(BF16)

    def block(index):
        return pl.ds(pl.multiple_of(index * CHUNK_ROWS, CHUNK_ROWS), CHUNK_ROWS)

    def group(g, half=None):
        if half is None:
            return pl.ds(pl.multiple_of(g * Z_ROWS, Z_ROWS), Z_ROWS)
        return pl.ds(pl.multiple_of(g * Z_ROWS + half * (Z_ROWS // 2), Z_ROWS // 2), Z_ROWS // 2)

    pltpu.make_async_copy(packed.at[block(me)], rows_in.at[x, block(me)], a_recv.at[z]).start()

    def dispatch(n, _):
        where, index = peer(n // 8, lax.rem(n, 8))
        send(packed.at[block(index)], rows_in.at[x, block(me)], a_send, a_recv.at[z], where)
        return 0

    lax.fori_loop(1, 64, dispatch, 0)

    await_(held.at[0, 0, pl.ds(0, NZ - 1)], own_send)
    await_(held.at[0, pl.ds(0, NY - 1)], fwd_send)
    for g in range(NY):
        await_(held.at[c, g], pair_send.at[g])
    for name in ("gate", "up"):
        loads[name].wait()
    for side, _other, origin in sides:
        await_(down_ref.at[origin, pl.ds(half_ff * (1 - side), half_ff)], d_recv.at[side, 1 - side])
        await_(down_ref.at[across, pl.ds(half_ff * side, half_ff)], h_recv.at[side])
    await_(down_ref.at[pl.ds(0, 2)], d_send)
    await_(down_ref.at[0], h_send)

    def turn(t, _):
        @pl.when(t < NZ)
        def _():
            g = group_of(t)
            ref = rows_in.at[x, group(g)]
            await_(ref, a_recv.at[g])
            for side, other, _origin in sides:
                send(ref, ref, b_send, b_recv.at[side, g], {"tp": other})

        @pl.when((t >= 1) & (t < NZ + 1))
        def _():
            g = group_of(t - 1)
            for side, other, origin in sides:
                await_(rows_in.at[origin, group(g)], b_recv.at[side, g])
                ref = rows_in.at[origin, group(g, side)]
                send(ref, ref, f_send, f_recv.at[side, g], {"tp": other})

        @pl.when((t >= 2) & (t < NZ + 2))
        def _():
            g = group_of(t - 2)
            for side, _other, _origin in sides:
                await_(rows_in.at[across, group(g, side)], f_recv.at[side, g])
            chunks = jnp.concatenate([rows_in[s, group(g)] for s in range(4)], axis=0)
            rows = from_chunks(chunks, swap_ref[...])
            gate = jnp.minimum(jnp.dot(rows, gate_ref[...], preferred_element_type=F32), CLAMP)
            lift = jnp.clip(jnp.dot(rows, up_ref[...], preferred_element_type=F32), -CLAMP, CLAMP)
            active = gate * jax.nn.sigmoid(ALPHA * gate) * (lift + 1.0)
            filler = jnp.zeros((ACT_ROWS - 24, FF_BLOCK), F32)
            for s in range(4):
                own_rows = jnp.concatenate([active[24 * s : 24 * s + 24], filler], axis=0)
                act_out[g, s] = own_rows.astype(BF16)
            act_in[g, x] = act_out[g, x]
            for n, other in enumerate((after, before, across)):
                send(act_out.at[g, other], act_in.at[g, x], g_send, g_recv.at[n, g], {"tp": other})

        @pl.when(t >= 3)
        def _():
            g = group_of(t - 3)
            for n, origin in enumerate((before, after, across)):
                await_(act_in.at[g, origin], g_recv.at[n, g])
            acts = jnp.concatenate([act_in[g, s] for s in range(4)], axis=1)
            down = down_ref[...].reshape(4 * FF_BLOCK, WIDTH)
            result = jnp.dot(acts, down, preferred_element_type=F32).astype(BF16)
            back[group(g)] = to_chunks(result, swap_ref[...])[:Z_ROWS]

            def give(k, _):
                py, pc = lax.rem(y + k // 2, NY), lax.rem(c + k, 2)
                index = (g * NY + py) * 2 + pc

                @pl.when(index == me)
                def _():
                    pltpu.make_async_copy(back.at[block(me)], home.at[block(me)], e_recv.at[z]).start()

                @pl.when(index != me)
                def _():
                    where = {"sp_0": g, "sp_1": py, "sp_2": pc}
                    send(back.at[block(index)], home.at[block(me)], e_send, e_recv.at[z], where)

                return 0

            lax.fori_loop(0, 8, give, 0)

        return 0

    lax.fori_loop(0, NZ + STAGES - 1, turn, 0)

    for g in range(NZ):
        await_(home.at[group(g)], e_recv.at[g])
    results = from_chunks(home[...], swap_ref[...])
    combined = jnp.dot(mix_ref[0], results, preferred_element_type=F32) + jnp.dot(
        mix_ref[1], results, preferred_element_type=F32
    )
    out_ref[...] = (mid_ref[...].astype(F32) + combined).astype(BF16)

    most = pl.ds(0, ALL_ROWS - CHUNK_ROWS)
    await_(packed.at[most], a_send)
    await_(back.at[most], e_send)
    await_(rows_in.at[pl.ds(0, 2)], b_send)
    await_(rows_in.at[0], f_send)
    await_(act_in.at[pl.ds(0, 6)], g_send)


def layer(small, large):
    vmem = pl.BlockSpec(memory_space=pltpu.VMEM)
    anywhere = pl.BlockSpec(memory_space=pl.ANY)
    dma = pltpu.SemaphoreType.DMA
    res, qn, qr, lat, key, upk, upv, ow, gate, up, down = large
    held_in = [
        pltpu.VMEM(a.shape[-2:], BF16) for a in (res, qn, qr, lat, key, upk, upv, ow, gate, up)
    ]
    return pl.pallas_call(
        layer_kernel,
        out_shape=jax.ShapeDtypeStruct(res.shape[1:], BF16),
        in_specs=[vmem] * len(small) + [anywhere] * len(large),
        out_specs=vmem,
        scratch_shapes=held_in
        + [
            pltpu.VMEM((4,) + down.shape[1:], BF16),
            pltpu.VMEM((2, NY, NZ, 128, 128), BF16),
            pltpu.VMEM((QROWS, 256), BF16),
            pltpu.VMEM((GROUP, 256), BF16),
            pltpu.VMEM((VROWS, GROUP), BF16),
            pltpu.VMEM((QROWS // CHUNK, GROUP, CHUNK), F32),
            pltpu.VMEM((QROWS // CHUNK, GROUP, CHUNK), BF16),
            pltpu.VMEM((VROWS, QROWS), F32),
            pltpu.VMEM((1, QROWS), F32),
            pltpu.VMEM((TOK, WIDTH), BF16),
            pltpu.VMEM((ALL_ROWS, 128), BF16),
            pltpu.VMEM((4, ALL_ROWS, 128), BF16),
            pltpu.VMEM((NZ, 4, ACT_ROWS, FF_BLOCK), BF16),
            pltpu.VMEM((NZ, 4, ACT_ROWS, FF_BLOCK), BF16),
            pltpu.VMEM((ALL_ROWS, 128), BF16),
            pltpu.VMEM((ALL_ROWS, 128), BF16),
            pltpu.VMEM((256, 256), BF16),
            pltpu.VMEM((2, TOK, 2 * TOK), BF16),
            dma((len(large),)), dma, dma, dma((NY,)), dma, dma, dma, dma, dma, dma, dma,
            dma((NZ,)), dma((NY,)), dma((NY,)), dma((2, 2)), dma((2,)),
            dma((NZ,)), dma((2, NZ)), dma((2, NZ)), dma((3, NZ)), dma((NZ,)),
        ],
        compiler_params=pltpu.CompilerParams(
            collective_id=0, has_side_effects=True, vmem_limit_bytes=60 * 2**20
        ),
    )(*small, *large)


def local(
    residual,
    query_nope,
    query_rope,
    latent,
    rope_key,
    latent_gain,
    up_key,
    up_value,
    out_weight,
    ffn_gain,
    routes,
    route_weight,
    gate_weight,
    up_weight,
    down_weight,
):
    half = ROPE // 2
    inverse = (ROPE_BASE ** (-(np.arange(128) % half) * 2.0 / ROPE)).astype(np.float32)
    small = (
        latent_gain[None],
        ffn_gain[None],
        jnp.asarray(inverse)[None],
        jnp.swapaxes(routes, 1, 2),
        jnp.swapaxes(route_weight[0], 0, 1),
    )
    large = (
        residual, query_nope, query_rope, latent, jnp.swapaxes(rope_key, 1, 2),
        up_key, up_value, out_weight, gate_weight, up_weight, down_weight,
    )
    return layer(small, large)[None]


def solution(mesh):
    split = Mesh(mesh.devices.reshape(8, 4, 2, mesh.shape["tp"]), ("sp_0", "sp_1", "sp_2", "tp"))
    in_specs = (
        P("tp", SP, None),
        P("tp", SP, None),
        P("tp", SP, None),
        P("tp", SP, None),
        P("tp", SP, None),
        P(),
        P(),
        P(),
        P(),
        P(),
        P(None, SP, None),
        P("tp", SP, None),
        P(SP, None, "tp"),
        P(SP, None, "tp"),
        P(SP, "tp", None),
    )
    out_specs = P("tp", SP, None)
    return jax.shard_map(local, mesh=split, in_specs=in_specs, out_specs=out_specs, check_vma=False)
```

```python
import math

import jax
import jax.numpy as jnp
import numpy as np
from jax import lax
from jax.experimental import pallas as pl
from jax.experimental.pallas import tpu as pltpu
from jax.sharding import Mesh
from jax.sharding import PartitionSpec as P

HEADS = 16
NOPE = 64
ROPE = 32
VDIM = 64
LATENT = 128
TOPK = 2
SP = ("sp_0", "sp_1", "sp_2")

EPS = 1e-06
ROPE_BASE = 10000.0
CLAMP = 7.0
ALPHA = 1.702
NEG_BIG = -1e30
MESH = pl.DeviceIdType.MESH

F32 = jnp.float32
BF16 = jnp.bfloat16
NZ, NY = 8, 4
TOK = 96
GROUP = NZ * TOK
QROWS = HEADS * TOK
CHUNK = 512
VROWS = LATENT + 16
KEYS = 256
Z_ORDER = (1, 7, 2, 6, 3, 5, 4)
ROW_ORDER = (0, 1, 7, 2, 6, 5, 3, 4)
FF_BLOCK = 256
ACT_ROWS = 32


def nt_dot(a, b):
    return lax.dot_general(a, b, (((1,), (1,)), ((), ())), preferred_element_type=F32)


def iota(shape, dim):
    return lax.broadcasted_iota(jnp.int32, shape, dim)


def turned(x, cosine, sine):
    low = iota(x.shape, 1) % ROPE < ROPE // 2
    swapped = jnp.where(low, pltpu.roll(x, 128 - ROPE // 2, 1), pltpu.roll(x, ROPE // 2, 1))
    return x * cosine + swapped * sine


CHUNK_ROWS = 3 * 16
Z_ROWS = 8 * CHUNK_ROWS
ALL_ROWS = 64 * CHUNK_ROWS
WIDTH = 2048
STAGES = 4


def mixed_tiles(x, outer, inner):
    return jnp.concatenate(
        [
            jnp.concatenate(
                [x[16 * a : 16 * a + 16, 128 * j : 128 * j + 128] for a in range(outer)], axis=1
            )
            for j in range(inner)
        ],
        axis=0,
    )


def side_by_side(x):
    return jnp.concatenate([x[256 * a : 256 * a + 256] for a in range(x.shape[0] // 256)], axis=1)


def stacked(x):
    return jnp.concatenate([x[:, 128 * a : 128 * a + 128] for a in range(x.shape[1] // 128)], axis=0)


def swap_matrix():
    row, col = iota((256, 256), 0), iota((256, 256), 1)
    return jnp.where(col == (row % 16) * 16 + row // 16, 1.0, 0.0).astype(BF16)


def to_chunks(rows, swap):
    mixed = mixed_tiles(rows, rows.shape[0] // 16, 16)
    return stacked(jnp.dot(swap, mixed, preferred_element_type=F32).astype(BF16))


def from_chunks(chunks, swap):
    mixed = jnp.dot(swap, side_by_side(chunks), preferred_element_type=F32).astype(BF16)
    return mixed_tiles(mixed, 16, chunks.shape[0] // 256)


def layer_kernel(
    gain_hbm, fgain_hbm, inv_hbm, routes_hbm, rw_hbm, res_hbm, qn_hbm, qr_hbm, lat_hbm, key_hbm, upk_hbm, upv_hbm, ow_hbm, gate_hbm, up_hbm, down_hbm,
    out_ref,
    gain_ref, fgain_ref, inv_ref, routes_ref, rw_ref, res_ref, qn_ref, qr_ref, lat_ref, key_ref, upk_ref, upv_ref, ow_ref, gate_ref, up_ref, down_ref,
    held, q_ref, k_ref, v_ref, s_ref, p_ref, acc_ref, peak_ref,
    mid_ref, packed, rows_in, act_out, act_in, back, home, swap_ref, mix_ref,
    in_sem, own_send, fwd_send, pair_send, d_send, h_send, a_send, b_send, f_send, g_send, e_send,
    z_recv, y_recv, pair_recv, d_recv, h_recv, a_recv, b_recv, f_recv, g_recv, e_recv,
):
    z, y, c = (lax.axis_index(name) for name in SP)
    x = lax.axis_index("tp")
    me = (z * NY + y) * 2 + c
    after, before, across = (lax.rem(x + d, 4) for d in (1, 3, 2))
    sides = ((0, after, before), (1, before, after))
    barrier = pltpu.get_barrier_semaphore()

    def distance(step):
        dz = 0
        for n, d in enumerate(ROW_ORDER):
            dz = dz + jnp.where(step == n, d, 0)
        return dz

    def peer(step, k):
        pz = lax.rem(z + distance(step), NZ)
        py, pc = lax.rem(y + k // 2, NY), lax.rem(c + k, 2)
        return {"sp_0": pz, "sp_1": py, "sp_2": pc}, (pz * NY + py) * 2 + pc

    def group_of(step):
        return lax.rem(z + NZ - distance(step), NZ)

    near = [{"sp_0": lax.rem(z + d, NZ)} for d in Z_ORDER]
    near += [{"sp_1": lax.rem(y + d, NY)} for d in (1, 3, 2)] + [{"sp_2": 1 - c}]
    near += [{"tp": other} for other in (after, before, across)]
    for where in near:
        pl.semaphore_signal(barrier, inc=1, device_id=where, device_id_type=MESH)

    loads = {}
    for n, (name, src, dst) in enumerate((
        ("inv", inv_hbm, inv_ref),
        ("gain", gain_hbm, gain_ref),
        ("lat", lat_hbm.at[0], lat_ref),
        ("key", key_hbm.at[0], key_ref),
        ("down", down_hbm.at[0], down_ref.at[x]),
        ("qn", qn_hbm.at[0], qn_ref),
        ("qr", qr_hbm.at[0], qr_ref),
        ("upk", upk_hbm, upk_ref),
        ("upv", upv_hbm, upv_ref),
        ("res", res_hbm.at[0], res_ref),
        ("ow", ow_hbm, ow_ref),
        ("gate", gate_hbm.at[0], gate_ref),
        ("up", up_hbm.at[0], up_ref),
        ("fgain", fgain_hbm, fgain_ref),
        ("routes", routes_hbm, routes_ref),
        ("rw", rw_hbm, rw_ref),
    )):
        loads[name] = pltpu.make_async_copy(src, dst, in_sem.at[n])
        loads[name].start()

    def await_(ref, sem):
        pltpu.make_async_copy(ref, ref, sem).wait()

    def send(src, dst, ssem, rsem, where):
        pltpu.make_async_remote_copy(
            src_ref=src, dst_ref=dst, send_sem=ssem, recv_sem=rsem,
            device_id=where, device_id_type=MESH,
        ).start()

    row, lane = iota((128, 128), 0), iota((128, 128), 1)
    token = jnp.where(row < TOK, row, row - TOK + 32 * (lane // ROPE))
    loads["inv"].wait()
    loads["gain"].wait()
    angle = (me * TOK + token).astype(F32) * inv_ref[...]
    cosine = jnp.cos(angle)
    sine = jnp.where(lane % ROPE < ROPE // 2, -1.0, 1.0) * jnp.sin(angle)

    loads["lat"].wait()
    wide = lat_ref[...].astype(F32)
    scale = lax.rsqrt(jnp.mean(wide * wide, axis=-1, keepdims=True) + EPS)
    held[c, y, z, :TOK, :] = (wide * scale * gain_ref[...]).astype(BF16)
    loads["key"].wait()
    raw = key_ref[...]
    keys = jnp.zeros((32, 128), F32)
    for j in range(TOK // 32):
        chosen = jnp.where(iota((32, TOK), 1) == 32 * j + iota((32, TOK), 0), 1.0, 0.0)
        blank = [jnp.zeros((32, TOK), BF16)] * 4
        blank[j] = raw
        keys = keys + nt_dot(chosen.astype(BF16), jnp.concatenate(blank, axis=0))
    held[c, y, z, TOK:, :] = turned(keys, cosine[TOK:], sine[TOK:]).astype(BF16)

    pl.semaphore_wait(barrier, len(near))

    loads["down"].wait()
    half_ff = FF_BLOCK // 2
    for side, other, _origin in sides:
        for h in (side, 1 - side):
            piece = down_ref.at[x, pl.ds(half_ff * h, half_ff)]
            send(piece, piece, d_send, d_recv.at[side, h], {"tp": other})

    def to_y(block, source):
        for d in (1, 3):
            where = {"sp_1": lax.rem(y + d, NY)}
            send(block, block, fwd_send, y_recv.at[y, source // (NZ // 2)], where)

    mine = held.at[c, y, z]
    for d in Z_ORDER:
        send(mine, mine, own_send, z_recv.at[z], {"sp_0": lax.rem(z + d, NZ)})
    to_y(mine, z)

    fold = (NOPE + ROPE) ** (-0.5) * math.log2(math.e)
    lane = iota((TOK, 128), 1)
    in_lane, out_lane = iota((128, 128), 0), iota((128, 128), 1)
    for name in ("qn", "qr", "upk"):
        loads[name].wait()
    turned_tiles = []
    for t in range(HEADS * ROPE // 128):
        tile = qr_ref[:, 128 * t : 128 * t + 128].astype(F32)
        turned_tiles.append((turned(tile, cosine[:TOK], sine[:TOK]) * fold).astype(BF16))
    pick = [
        jnp.where((out_lane < TOK) & (in_lane == ROPE * m + out_lane % ROPE), 1.0, 0.0).astype(BF16)
        for m in range(4)
    ]
    for h in range(HEADS):
        t = h // 2
        plain = qn_ref[:, 128 * t : 128 * t + 128]
        half = lane < NOPE if h % 2 == 0 else lane >= NOPE
        plain = jnp.where(half, plain, jnp.zeros_like(plain))
        lifted = nt_dot(plain, upk_ref[:, 128 * t : 128 * t + 128]) * fold
        q_ref[TOK * h : TOK * h + TOK, :128] = lifted.astype(BF16)
        rotary = jnp.dot(turned_tiles[h // 4], pick[h % 4], preferred_element_type=F32)
        q_ref[TOK * h : TOK * h + TOK, 128:] = rotary.astype(BF16)

    acc_ref[...] = jnp.zeros_like(acc_ref)
    peak_ref[...] = jnp.full_like(peak_ref, NEG_BIG)
    v_ref[LATENT:, :] = jnp.ones((VROWS - LATENT, GROUP), BF16)
    swap_ref[...] = swap_matrix()

    for d in Z_ORDER:
        source = lax.rem(z + d, NZ)
        block = held.at[c, y, source]
        await_(block, z_recv.at[source])
        to_y(block, source)

    def step(s, _):
        dy = jnp.where(s < 2, 0, jnp.where(s >= 6, 2, jnp.where(lax.rem(s, 2) == 0, 1, 3)))
        gy = lax.rem(y + dy, NY)
        own = (s == 0) | (s == 2) | (s == 3) | (s == 6)
        gc = jnp.where(own, c, 1 - c)
        group = held.at[gc, gy]

        def half_column(origin, h):
            return held.at[c, origin, pl.ds(h * (NZ // 2), NZ // 2)]

        @pl.when(s == 2)
        def _():
            for h, d in ((0, 1), (1, 3)):
                origin = lax.rem(y + NY - d, NY)
                part = half_column(origin, h)
                await_(part, y_recv.at[origin, h])
                send(part, part, fwd_send, y_recv.at[origin, h], {"sp_1": lax.rem(y + d, NY)})

        @pl.when((s == 2) | (s == 6))
        def _():
            await_(half_column(gy, 0), y_recv.at[gy, 0])

        @pl.when((s == 3) | (s == 6))
        def _():
            await_(half_column(gy, 1), y_recv.at[gy, 1])

        @pl.when(own)
        def _():
            send(group, group, pair_send.at[gy], pair_recv.at[gy], {"sp_2": 1 - c})

        @pl.when(jnp.logical_not(own))
        def _():
            await_(group, pair_recv.at[gy])

        @pl.when(s == 4)
        def _():
            for side, other, origin in sides:
                piece = down_ref.at[origin, pl.ds(half_ff * side, half_ff)]
                await_(piece, d_recv.at[side, side])
                send(piece, piece, h_send, h_recv.at[side], {"tp": other})

        lane32 = iota((32, 128), 1) // ROPE
        for b in range(NZ):
            k_ref[TOK * b : TOK * b + TOK, :128] = held[gc, gy, b, :TOK, :]
            packed_keys = held[gc, gy, b, TOK:, :]
            for j in range(TOK // 32):
                first = TOK * b + 32 * j
                k_ref[first : first + 32, 128:] = jnp.where(
                    lane32 == j, packed_keys, jnp.zeros_like(packed_keys)
                )
        for b in range(GROUP // 128):
            v_ref[:LATENT, 128 * b : 128 * b + 128] = k_ref[128 * b : 128 * b + 128, :128].T

        def cols(n):
            return slice(CHUNK * n, CHUNK * n + CHUNK)

        def score(n, r):
            keys = slice(KEYS * r, KEYS * r + KEYS)
            made = nt_dot(k_ref[keys, :], q_ref[cols(n), :])
            s_ref[n, keys, :] = made
            return jnp.max(made.reshape(KEYS // 8, 8, CHUNK), axis=0)

        def raised(n, tops):
            old = peak_ref[:, cols(n)]
            most = jnp.maximum(jnp.maximum(tops[0], tops[1]), tops[2])
            top = jnp.maximum(old, jnp.max(most, axis=0, keepdims=True))
            peak_ref[:, cols(n)] = top
            return top, jnp.exp2(old - top)

        def weigh(n, r, top):
            keys = slice(KEYS * r, KEYS * r + KEYS)
            p_ref[n, keys, :] = jnp.exp2(s_ref[n, keys, :] - top).astype(BF16)

        def mix(n, shrink):
            mixed = jnp.dot(v_ref[...], p_ref[n], preferred_element_type=F32)
            acc_ref[:, cols(n)] = acc_ref[:, cols(n)] * shrink + mixed

        blocks = range(GROUP // KEYS)
        chunks = QROWS // CHUNK
        top, shrink = raised(0, [score(0, r) for r in blocks])
        for n in range(1, chunks + 1):
            tops = []
            for r in blocks:
                if n < chunks:
                    tops.append(score(n, r))
                weigh(n - 1, r, top)
            mix(n - 1, shrink)
            if n < chunks:
                top, shrink = raised(n, tops)
        return 0

    lax.fori_loop(0, 2 * NY, step, 0)

    lat_t = acc_ref[:LATENT, :] / acc_ref[LATENT : LATENT + 1, :]
    mixed_rows = jnp.concatenate(
        [lat_t[:, 128 * b : 128 * b + 128].T for b in range(QROWS // 128)], axis=0
    ).astype(BF16)
    tiles = []
    loads["upv"].wait()
    for t in range(HEADS // 2):
        up = upv_ref[:, 128 * t : 128 * t + 128]
        even = jnp.dot(mixed_rows[192 * t : 192 * t + 96], up, preferred_element_type=F32)
        odd = jnp.dot(mixed_rows[192 * t + 96 : 192 * t + 192], up, preferred_element_type=F32)
        tiles.append(jnp.where(lane < VDIM, even, odd).astype(BF16))
    attended = jnp.concatenate(tiles, axis=1)
    for name in ("ow", "res", "fgain", "routes", "rw"):
        loads[name].wait()
    projected = jnp.dot(attended, ow_ref[...], preferred_element_type=F32)
    middle = (res_ref[...].astype(F32) + projected).astype(BF16)
    mid_ref[...] = middle
    wide = middle.astype(F32)
    scale = lax.rsqrt(jnp.mean(wide * wide, axis=-1, keepdims=True) + EPS)
    normal_rows = (wide * scale * fgain_ref[...]).astype(BF16)

    picks = routes_ref[x].astype(F32)
    down_i, right_i = iota((TOK, TOK), 0), iota((TOK, TOK), 1)

    def as_column(line):
        return jnp.sum(jnp.where(down_i == right_i, line, 0.0), axis=1, keepdims=True)

    row = [picks[k : k + 1, :] for k in range(TOPK)]
    col = [as_column(line) for line in row]
    earlier_r = jnp.where(down_i < right_i, 1.0, 0.0)
    earlier_c = jnp.where(right_i < down_i, 1.0, 0.0)

    def same(a, b):
        return jnp.where(a == b, 1.0, 0.0)

    rank_row = [
        jnp.sum(same(col[0], row[0]) * earlier_r, axis=0, keepdims=True),
        jnp.sum(same(col[0], row[1]) + same(col[1], row[1]) * earlier_r, axis=0, keepdims=True),
    ]
    rank_col = [
        jnp.sum(same(row[0], col[0]) * earlier_c, axis=1, keepdims=True),
        jnp.sum(same(row[0], col[1]) + same(row[1], col[1]) * earlier_c, axis=1, keepdims=True),
    ]
    slot_d = iota((2 * TOK, TOK), 0).astype(F32)
    spread = sum(same(slot_d, 3.0 * row[k] + rank_row[k]) for k in range(TOPK)).astype(BF16)
    sent = jnp.dot(spread, normal_rows, preferred_element_type=F32).astype(BF16)
    packed[...] = to_chunks(sent, swap_ref[...])
    slot_c = iota((TOK, 2 * TOK), 1).astype(F32)
    weight = sum(
        same(slot_c, 3.0 * col[k] + rank_col[k]) * as_column(rw_ref[k : k + 1, :])
        for k in range(TOPK)
    )
    high = weight.astype(BF16)
    mix_ref[0] = high
    mix_ref[1] = (weight - high.astype(F32)).astype(BF16)

    def block(index):
        return pl.ds(pl.multiple_of(index * CHUNK_ROWS, CHUNK_ROWS), CHUNK_ROWS)

    def group(g, half=None):
        if half is None:
            return pl.ds(pl.multiple_of(g * Z_ROWS, Z_ROWS), Z_ROWS)
        first = 3 * CHUNK_ROWS
        if half == 0:
            return pl.ds(pl.multiple_of(g * Z_ROWS, CHUNK_ROWS), first)
        return pl.ds(pl.multiple_of(g * Z_ROWS + first, CHUNK_ROWS), Z_ROWS - first)

    pltpu.make_async_copy(packed.at[block(me)], rows_in.at[x, block(me)], a_recv.at[z]).start()

    def dispatch(n, _):
        where, index = peer(n // 8, lax.rem(n, 8))

        @pl.when(index != me)
        def _():
            send(packed.at[block(index)], rows_in.at[x, block(me)], a_send, a_recv.at[z], where)

        return 0

    lax.fori_loop(0, 64, dispatch, 0)

    for name in ("gate", "up"):
        loads[name].wait()

    def turn(t, _):
        @pl.when(t < NZ)
        def _():
            g = group_of(t)
            ref = rows_in.at[x, group(g)]
            await_(ref, a_recv.at[g])
            for side, other, _origin in sides:
                send(ref, ref, b_send, b_recv.at[side, g], {"tp": other})

        @pl.when((t >= 1) & (t < NZ + 1))
        def _():
            g = group_of(t - 1)
            for side, other, origin in sides:
                await_(rows_in.at[origin, group(g)], b_recv.at[side, g])
                ref = rows_in.at[origin, group(g, side)]
                send(ref, ref, f_send, f_recv.at[side, g], {"tp": other})

        @pl.when((t >= 2) & (t < NZ + 2))
        def _():
            g = group_of(t - 2)
            for side, _other, _origin in sides:
                await_(rows_in.at[across, group(g, side)], f_recv.at[side, g])
            chunks = jnp.concatenate([rows_in[s, group(g)] for s in range(4)], axis=0)
            rows = from_chunks(chunks, swap_ref[...])
            gate = jnp.minimum(jnp.dot(rows, gate_ref[...], preferred_element_type=F32), CLAMP)
            lift = jnp.clip(jnp.dot(rows, up_ref[...], preferred_element_type=F32), -CLAMP, CLAMP)
            active = gate * jax.nn.sigmoid(ALPHA * gate) * (lift + 1.0)
            filler = jnp.zeros((ACT_ROWS - 24, FF_BLOCK), F32)
            for s in range(4):
                own_rows = jnp.concatenate([active[24 * s : 24 * s + 24], filler], axis=0)
                act_out[g, s] = own_rows.astype(BF16)
            act_in[g, x] = act_out[g, x]
            for n, other in enumerate((after, before, across)):
                send(act_out.at[g, other], act_in.at[g, x], g_send, g_recv.at[n, g], {"tp": other})

        @pl.when(t >= 3)
        def _():
            g = group_of(t - 3)

            @pl.when(t == 3)
            def _():
                for side, _other, origin in sides:
                    rest = pl.ds(half_ff * (1 - side), half_ff)
                    await_(down_ref.at[origin, rest], d_recv.at[side, 1 - side])
                    await_(down_ref.at[across, pl.ds(half_ff * side, half_ff)], h_recv.at[side])

            for n, origin in enumerate((before, after, across)):
                await_(act_in.at[g, origin], g_recv.at[n, g])
            acts = jnp.concatenate([act_in[g, s] for s in range(4)], axis=1)
            down = down_ref[...].reshape(4 * FF_BLOCK, WIDTH)
            result = jnp.dot(acts, down, preferred_element_type=F32).astype(BF16)
            back[group(g)] = to_chunks(result, swap_ref[...])[:Z_ROWS]

            def give(k, _):
                py, pc = lax.rem(y + k // 2, NY), lax.rem(c + k, 2)
                index = (g * NY + py) * 2 + pc

                @pl.when(index == me)
                def _():
                    pltpu.make_async_copy(back.at[block(me)], home.at[block(me)], e_recv.at[z]).start()

                @pl.when(index != me)
                def _():
                    where = {"sp_0": g, "sp_1": py, "sp_2": pc}
                    send(back.at[block(index)], home.at[block(me)], e_send, e_recv.at[z], where)

                return 0

            lax.fori_loop(0, 8, give, 0)

        return 0

    lax.fori_loop(0, NZ + STAGES - 1, turn, 0)

    for g in range(NZ):
        await_(home.at[group(g)], e_recv.at[g])
    results = from_chunks(home[...], swap_ref[...])
    combined = jnp.dot(mix_ref[0], results, preferred_element_type=F32) + jnp.dot(
        mix_ref[1], results, preferred_element_type=F32
    )
    out_ref[...] = (mid_ref[...].astype(F32) + combined).astype(BF16)

    await_(held.at[0, 0, pl.ds(0, NZ - 1)], own_send)
    await_(held.at[0, pl.ds(0, NY - 1)], fwd_send)
    for g in range(NY):
        await_(held.at[c, g], pair_send.at[g])
    await_(down_ref.at[pl.ds(0, 2)], d_send)
    await_(down_ref.at[0], h_send)
    most = pl.ds(0, ALL_ROWS - CHUNK_ROWS)
    await_(packed.at[most], a_send)
    await_(back.at[most], e_send)
    await_(rows_in.at[pl.ds(0, 2)], b_send)
    await_(rows_in.at[0], f_send)
    await_(act_in.at[pl.ds(0, 6)], g_send)


def layer(small, large):
    vmem = pl.BlockSpec(memory_space=pltpu.VMEM)
    anywhere = pl.BlockSpec(memory_space=pl.ANY)
    dma = pltpu.SemaphoreType.DMA
    res, qn, qr, lat, key, upk, upv, ow, gate, up, down = large
    held_in = [
        pltpu.VMEM(a.shape[-2:], BF16) for a in (res, qn, qr, lat, key, upk, upv, ow, gate, up)
    ]
    return pl.pallas_call(
        layer_kernel,
        out_shape=jax.ShapeDtypeStruct(res.shape[1:], BF16),
        in_specs=[anywhere] * (len(small) + len(large)),
        out_specs=vmem,
        scratch_shapes=[pltpu.VMEM(a.shape, a.dtype) for a in small]
        + held_in
        + [
            pltpu.VMEM((4,) + down.shape[1:], BF16),
            pltpu.VMEM((2, NY, NZ, 128, 128), BF16),
            pltpu.VMEM((QROWS, 256), BF16),
            pltpu.VMEM((GROUP, 256), BF16),
            pltpu.VMEM((VROWS, GROUP), BF16),
            pltpu.VMEM((QROWS // CHUNK, GROUP, CHUNK), F32),
            pltpu.VMEM((QROWS // CHUNK, GROUP, CHUNK), BF16),
            pltpu.VMEM((VROWS, QROWS), F32),
            pltpu.VMEM((1, QROWS), F32),
            pltpu.VMEM((TOK, WIDTH), BF16),
            pltpu.VMEM((ALL_ROWS, 128), BF16),
            pltpu.VMEM((4, ALL_ROWS, 128), BF16),
            pltpu.VMEM((NZ, 4, ACT_ROWS, FF_BLOCK), BF16),
            pltpu.VMEM((NZ, 4, ACT_ROWS, FF_BLOCK), BF16),
            pltpu.VMEM((ALL_ROWS, 128), BF16),
            pltpu.VMEM((ALL_ROWS, 128), BF16),
            pltpu.VMEM((256, 256), BF16),
            pltpu.VMEM((2, TOK, 2 * TOK), BF16),
            dma((len(small) + len(large),)), dma, dma, dma((NY,)), dma, dma, dma, dma, dma, dma, dma,
            dma((NZ,)), dma((NY, 2)), dma((NY,)), dma((2, 2)), dma((2,)),
            dma((NZ,)), dma((2, NZ)), dma((2, NZ)), dma((3, NZ)), dma((NZ,)),
        ],
        compiler_params=pltpu.CompilerParams(
            collective_id=0, has_side_effects=True, vmem_limit_bytes=60 * 2**20
        ),
    )(*small, *large)


def local(
    residual,
    query_nope,
    query_rope,
    latent,
    rope_key,
    latent_gain,
    up_key,
    up_value,
    out_weight,
    ffn_gain,
    routes,
    route_weight,
    gate_weight,
    up_weight,
    down_weight,
):
    half = ROPE // 2
    inverse = (ROPE_BASE ** (-(np.arange(128) % half) * 2.0 / ROPE)).astype(np.float32)
    small = (
        latent_gain[None],
        ffn_gain[None],
        jnp.asarray(inverse)[None],
        jnp.swapaxes(routes, 1, 2),
        jnp.swapaxes(route_weight[0], 0, 1),
    )
    large = (
        residual, query_nope, query_rope, latent, jnp.swapaxes(rope_key, 1, 2),
        up_key, up_value, out_weight, gate_weight, up_weight, down_weight,
    )
    return layer(small, large)[None]


def solution(mesh):
    split = Mesh(mesh.devices.reshape(8, 4, 2, mesh.shape["tp"]), ("sp_0", "sp_1", "sp_2", "tp"))
    in_specs = (
        P("tp", SP, None),
        P("tp", SP, None),
        P("tp", SP, None),
        P("tp", SP, None),
        P("tp", SP, None),
        P(),
        P(),
        P(),
        P(),
        P(),
        P(None, SP, None),
        P("tp", SP, None),
        P(SP, None, "tp"),
        P(SP, None, "tp"),
        P(SP, "tp", None),
    )
    out_specs = P("tp", SP, None)
    return jax.shard_map(local, mesh=split, in_specs=in_specs, out_specs=out_specs, check_vma=False)
```

```python
import math

import jax
import jax.numpy as jnp
import numpy as np
from jax import lax
from jax.experimental import pallas as pl
from jax.experimental.pallas import tpu as pltpu
from jax.sharding import Mesh
from jax.sharding import PartitionSpec as P

HEADS = 16
NOPE = 64
ROPE = 32
VDIM = 64
LATENT = 128
TOPK = 2
SP = ("sp_0", "sp_1", "sp_2")

EPS = 1e-06
ROPE_BASE = 10000.0
CLAMP = 7.0
ALPHA = 1.702
NEG_BIG = -1e30
MESH = pl.DeviceIdType.MESH

F32 = jnp.float32
BF16 = jnp.bfloat16
NZ, NY = 8, 4
TOK = 96
GROUP = NZ * TOK
QROWS = HEADS * TOK
CHUNK = 512
VROWS = LATENT + 16
KEYS = 256
Z_ORDER = (1, 7, 2, 6, 3, 5, 4)
ROW_ORDER = (0, 7, 6, 2, 5, 3, 4, 1)
FF_BLOCK = 256
OWN_ROWS = 24


def nt_dot(a, b):
    return lax.dot_general(a, b, (((1,), (1,)), ((), ())), preferred_element_type=F32)


def iota(shape, dim):
    return lax.broadcasted_iota(jnp.int32, shape, dim)


def turned(x, cosine, sine):
    low = iota(x.shape, 1) % ROPE < ROPE // 2
    swapped = jnp.where(low, pltpu.roll(x, 128 - ROPE // 2, 1), pltpu.roll(x, ROPE // 2, 1))
    return x * cosine + swapped * sine


CHUNK_ROWS = 3 * 16
Z_ROWS = 8 * CHUNK_ROWS
ALL_ROWS = 64 * CHUNK_ROWS
WIDTH = 2048
STAGES = 4


def mixed_tiles(x, outer, inner):
    return jnp.concatenate(
        [
            jnp.concatenate(
                [x[16 * a : 16 * a + 16, 128 * j : 128 * j + 128] for a in range(outer)], axis=1
            )
            for j in range(inner)
        ],
        axis=0,
    )


def side_by_side(x):
    return jnp.concatenate([x[256 * a : 256 * a + 256] for a in range(x.shape[0] // 256)], axis=1)


def stacked(x):
    return jnp.concatenate([x[:, 128 * a : 128 * a + 128] for a in range(x.shape[1] // 128)], axis=0)


def swap_matrix():
    row, col = iota((256, 256), 0), iota((256, 256), 1)
    return jnp.where(col == (row % 16) * 16 + row // 16, 1.0, 0.0).astype(BF16)


def to_chunks(rows, swap):
    mixed = mixed_tiles(rows, rows.shape[0] // 16, 16)
    return stacked(jnp.dot(swap, mixed, preferred_element_type=F32).astype(BF16))


def from_chunks(chunks, swap):
    mixed = jnp.dot(swap, side_by_side(chunks), preferred_element_type=F32).astype(BF16)
    return mixed_tiles(mixed, 16, chunks.shape[0] // 256)


def layer_kernel(
    gain_hbm, fgain_hbm, inv_hbm, routes_hbm, rw_hbm, res_hbm, qn_hbm, qr_hbm, lat_hbm, key_hbm, upk_hbm, upv_hbm, ow_hbm, gate_hbm, up_hbm, down_hbm,
    out_ref,
    gain_ref, fgain_ref, inv_ref, routes_ref, rw_ref, res_ref, qn_ref, qr_ref, lat_ref, key_ref, upk_ref, upv_ref, ow_ref, gate_ref, up_ref, down_ref,
    held, q_ref, k_ref, v_ref, s_ref, p_ref, acc_ref, peak_ref,
    mid_ref, packed, rows_in, act_out, act_in, back, home, swap_ref, mix_ref,
    in_sem, own_send, fwd_send, pair_send, d_send, h_send, a_send, b_send, f_send, g_send, e_send,
    z_recv, y_recv, pair_recv, d_recv, h_recv, a_recv, b_recv, f_recv, g_recv, e_recv,
):
    z, y, c = (lax.axis_index(name) for name in SP)
    x = lax.axis_index("tp")
    me = (z * NY + y) * 2 + c
    after, before, across = (lax.rem(x + d, 4) for d in (1, 3, 2))
    sides = ((0, after, before), (1, before, after))
    barrier = pltpu.get_barrier_semaphore()

    def distance(step):
        dz = 0
        for n, d in enumerate(ROW_ORDER):
            dz = dz + jnp.where(step == n, d, 0)
        return dz

    def peer(step, k):
        pz = lax.rem(z + distance(step), NZ)
        py, pc = lax.rem(y + k // 2, NY), lax.rem(c + k, 2)
        return {"sp_0": pz, "sp_1": py, "sp_2": pc}, (pz * NY + py) * 2 + pc

    def group_of(step):
        return lax.rem(z + NZ - distance(step), NZ)

    near = [{"sp_0": lax.rem(z + d, NZ)} for d in Z_ORDER]
    near += [{"sp_1": lax.rem(y + d, NY)} for d in (1, 3, 2)] + [{"sp_2": 1 - c}]
    near += [{"tp": other} for other in (after, before, across)]
    for where in near:
        pl.semaphore_signal(barrier, inc=1, device_id=where, device_id_type=MESH)

    loads = {}
    for n, (name, src, dst) in enumerate((
        ("inv", inv_hbm, inv_ref),
        ("gain", gain_hbm, gain_ref),
        ("lat", lat_hbm.at[0], lat_ref),
        ("key", key_hbm.at[0], key_ref),
        ("down", down_hbm.at[0], down_ref.at[x]),
        ("qn", qn_hbm.at[0], qn_ref),
        ("qr", qr_hbm.at[0], qr_ref),
        ("upk", upk_hbm, upk_ref),
        ("upv", upv_hbm, upv_ref),
        ("res", res_hbm.at[0], res_ref),
        ("ow", ow_hbm, ow_ref),
        ("gate", gate_hbm.at[0], gate_ref),
        ("up", up_hbm.at[0], up_ref),
        ("fgain", fgain_hbm, fgain_ref),
        ("routes", routes_hbm, routes_ref),
        ("rw", rw_hbm, rw_ref),
    )):
        loads[name] = pltpu.make_async_copy(src, dst, in_sem.at[n])
        loads[name].start()

    def await_(ref, sem):
        pltpu.make_async_copy(ref, ref, sem).wait()

    def send(src, dst, ssem, rsem, where):
        pltpu.make_async_remote_copy(
            src_ref=src, dst_ref=dst, send_sem=ssem, recv_sem=rsem,
            device_id=where, device_id_type=MESH,
        ).start()

    row, lane = iota((128, 128), 0), iota((128, 128), 1)
    token = jnp.where(row < TOK, row, row - TOK + 32 * (lane // ROPE))
    loads["inv"].wait()
    loads["gain"].wait()
    angle = (me * TOK + token).astype(F32) * inv_ref[...]
    cosine = jnp.cos(angle)
    sine = jnp.where(lane % ROPE < ROPE // 2, -1.0, 1.0) * jnp.sin(angle)

    loads["lat"].wait()
    wide = lat_ref[...].astype(F32)
    scale = lax.rsqrt(jnp.mean(wide * wide, axis=-1, keepdims=True) + EPS)
    held[c, y, z, :TOK, :] = (wide * scale * gain_ref[...]).astype(BF16)
    loads["key"].wait()
    raw = key_ref[...]
    keys = jnp.zeros((32, 128), F32)
    for j in range(TOK // 32):
        chosen = jnp.where(iota((32, TOK), 1) == 32 * j + iota((32, TOK), 0), 1.0, 0.0)
        blank = [jnp.zeros((32, TOK), BF16)] * 4
        blank[j] = raw
        keys = keys + nt_dot(chosen.astype(BF16), jnp.concatenate(blank, axis=0))
    held[c, y, z, TOK:, :] = turned(keys, cosine[TOK:], sine[TOK:]).astype(BF16)

    pl.semaphore_wait(barrier, len(near))

    loads["down"].wait()
    half_ff = FF_BLOCK // 2
    for side, other, _origin in sides:
        for h in (side, 1 - side):
            piece = down_ref.at[x, pl.ds(half_ff * h, half_ff)]
            send(piece, piece, d_send, d_recv.at[side, h], {"tp": other})

    def to_y(block, source):
        for d in (1, 3):
            where = {"sp_1": lax.rem(y + d, NY)}
            send(block, block, fwd_send, y_recv.at[y, source // (NZ // 2)], where)

    mine = held.at[c, y, z]
    for d in Z_ORDER:
        send(mine, mine, own_send, z_recv.at[z], {"sp_0": lax.rem(z + d, NZ)})
    to_y(mine, z)

    fold = (NOPE + ROPE) ** (-0.5) * math.log2(math.e)
    lane = iota((TOK, 128), 1)
    in_lane, out_lane = iota((128, 128), 0), iota((128, 128), 1)
    for name in ("qn", "qr", "upk"):
        loads[name].wait()
    turned_tiles = []
    for t in range(HEADS * ROPE // 128):
        tile = qr_ref[:, 128 * t : 128 * t + 128].astype(F32)
        turned_tiles.append((turned(tile, cosine[:TOK], sine[:TOK]) * fold).astype(BF16))
    pick = [
        jnp.where((out_lane < TOK) & (in_lane == ROPE * m + out_lane % ROPE), 1.0, 0.0).astype(BF16)
        for m in range(4)
    ]
    for h in range(HEADS):
        t = h // 2
        plain = qn_ref[:, 128 * t : 128 * t + 128]
        half = lane < NOPE if h % 2 == 0 else lane >= NOPE
        plain = jnp.where(half, plain, jnp.zeros_like(plain))
        lifted = nt_dot(plain, upk_ref[:, 128 * t : 128 * t + 128]) * fold
        q_ref[TOK * h : TOK * h + TOK, :128] = lifted.astype(BF16)
        rotary = jnp.dot(turned_tiles[h // 4], pick[h % 4], preferred_element_type=F32)
        q_ref[TOK * h : TOK * h + TOK, 128:] = rotary.astype(BF16)

    acc_ref[...] = jnp.zeros_like(acc_ref)
    peak_ref[...] = jnp.full_like(peak_ref, NEG_BIG)
    v_ref[LATENT:, :] = jnp.ones((VROWS - LATENT, GROUP), BF16)
    swap_ref[...] = swap_matrix()

    for d in Z_ORDER:
        source = lax.rem(z + d, NZ)
        block = held.at[c, y, source]
        await_(block, z_recv.at[source])
        to_y(block, source)

    def step(s, _):
        dy = jnp.where(s < 2, 0, jnp.where(s >= 6, 2, jnp.where(lax.rem(s, 2) == 0, 1, 3)))
        gy = lax.rem(y + dy, NY)
        own = (s == 0) | (s == 2) | (s == 3) | (s == 6)
        gc = jnp.where(own, c, 1 - c)
        group = held.at[gc, gy]

        def half_column(origin, h):
            return held.at[c, origin, pl.ds(h * (NZ // 2), NZ // 2)]

        @pl.when(s == 2)
        def _():
            for h, d in ((0, 1), (1, 3)):
                origin = lax.rem(y + NY - d, NY)
                part = half_column(origin, h)
                await_(part, y_recv.at[origin, h])
                send(part, part, fwd_send, y_recv.at[origin, h], {"sp_1": lax.rem(y + d, NY)})

        @pl.when((s == 2) | (s == 6))
        def _():
            await_(half_column(gy, 0), y_recv.at[gy, 0])

        @pl.when((s == 3) | (s == 6))
        def _():
            await_(half_column(gy, 1), y_recv.at[gy, 1])

        @pl.when(own)
        def _():
            send(group, group, pair_send.at[gy], pair_recv.at[gy], {"sp_2": 1 - c})

        @pl.when(jnp.logical_not(own))
        def _():
            await_(group, pair_recv.at[gy])

        @pl.when(s == 4)
        def _():
            for side, other, origin in sides:
                piece = down_ref.at[origin, pl.ds(half_ff * side, half_ff)]
                await_(piece, d_recv.at[side, side])
                send(piece, piece, h_send, h_recv.at[side], {"tp": other})

        lane32 = iota((32, 128), 1) // ROPE
        for b in range(NZ):
            k_ref[TOK * b : TOK * b + TOK, :128] = held[gc, gy, b, :TOK, :]
            packed_keys = held[gc, gy, b, TOK:, :]
            for j in range(TOK // 32):
                first = TOK * b + 32 * j
                k_ref[first : first + 32, 128:] = jnp.where(
                    lane32 == j, packed_keys, jnp.zeros_like(packed_keys)
                )
        for b in range(GROUP // 128):
            v_ref[:LATENT, 128 * b : 128 * b + 128] = k_ref[128 * b : 128 * b + 128, :128].T

        def cols(n):
            return slice(CHUNK * n, CHUNK * n + CHUNK)

        def score(n, r):
            keys = slice(KEYS * r, KEYS * r + KEYS)
            made = nt_dot(k_ref[keys, :], q_ref[cols(n), :])
            s_ref[n, keys, :] = made
            return jnp.max(made.reshape(KEYS // 8, 8, CHUNK), axis=0)

        def raised(n, tops):
            old = peak_ref[:, cols(n)]
            most = jnp.maximum(jnp.maximum(tops[0], tops[1]), tops[2])
            top = jnp.maximum(old, jnp.max(most, axis=0, keepdims=True))
            peak_ref[:, cols(n)] = top
            return top, jnp.exp2(old - top)

        def weigh(n, r, top):
            keys = slice(KEYS * r, KEYS * r + KEYS)
            p_ref[n, keys, :] = jnp.exp2(s_ref[n, keys, :] - top).astype(BF16)

        def mix(n, shrink):
            mixed = jnp.dot(v_ref[...], p_ref[n], preferred_element_type=F32)
            acc_ref[:, cols(n)] = acc_ref[:, cols(n)] * shrink + mixed

        blocks = range(GROUP // KEYS)
        chunks = QROWS // CHUNK
        top, shrink = raised(0, [score(0, r) for r in blocks])
        for n in range(1, chunks + 1):
            tops = []
            for r in blocks:
                if n < chunks:
                    tops.append(score(n, r))
                weigh(n - 1, r, top)
            mix(n - 1, shrink)
            if n < chunks:
                top, shrink = raised(n, tops)
        return 0

    lax.fori_loop(0, 2 * NY, step, 0)

    lat_t = acc_ref[:LATENT, :] / acc_ref[LATENT : LATENT + 1, :]
    mixed_rows = jnp.concatenate(
        [lat_t[:, 128 * b : 128 * b + 128].T for b in range(QROWS // 128)], axis=0
    ).astype(BF16)
    tiles = []
    loads["upv"].wait()
    for t in range(HEADS // 2):
        up = upv_ref[:, 128 * t : 128 * t + 128]
        even = jnp.dot(mixed_rows[192 * t : 192 * t + 96], up, preferred_element_type=F32)
        odd = jnp.dot(mixed_rows[192 * t + 96 : 192 * t + 192], up, preferred_element_type=F32)
        tiles.append(jnp.where(lane < VDIM, even, odd).astype(BF16))
    attended = jnp.concatenate(tiles, axis=1)
    for name in ("ow", "res", "fgain", "routes", "rw"):
        loads[name].wait()
    projected = jnp.dot(attended, ow_ref[...], preferred_element_type=F32)
    middle = (res_ref[...].astype(F32) + projected).astype(BF16)
    mid_ref[...] = middle
    wide = middle.astype(F32)
    scale = lax.rsqrt(jnp.mean(wide * wide, axis=-1, keepdims=True) + EPS)
    normal_rows = (wide * scale * fgain_ref[...]).astype(BF16)

    picks = routes_ref[x].astype(F32)
    down_i, right_i = iota((TOK, TOK), 0), iota((TOK, TOK), 1)

    def as_column(line):
        return jnp.sum(jnp.where(down_i == right_i, line, 0.0), axis=1, keepdims=True)

    row = [picks[k : k + 1, :] for k in range(TOPK)]
    col = [as_column(line) for line in row]
    earlier_r = jnp.where(down_i < right_i, 1.0, 0.0)
    earlier_c = jnp.where(right_i < down_i, 1.0, 0.0)

    def same(a, b):
        return jnp.where(a == b, 1.0, 0.0)

    rank_row = [
        jnp.sum(same(col[0], row[0]) * earlier_r, axis=0, keepdims=True),
        jnp.sum(same(col[0], row[1]) + same(col[1], row[1]) * earlier_r, axis=0, keepdims=True),
    ]
    rank_col = [
        jnp.sum(same(row[0], col[0]) * earlier_c, axis=1, keepdims=True),
        jnp.sum(same(row[0], col[1]) + same(row[1], col[1]) * earlier_c, axis=1, keepdims=True),
    ]
    slot_d = iota((2 * TOK, TOK), 0).astype(F32)
    spread = sum(same(slot_d, 3.0 * row[k] + rank_row[k]) for k in range(TOPK)).astype(BF16)
    sent = jnp.dot(spread, normal_rows, preferred_element_type=F32).astype(BF16)
    packed[...] = to_chunks(sent, swap_ref[...])
    slot_c = iota((TOK, 2 * TOK), 1).astype(F32)
    weight = sum(
        same(slot_c, 3.0 * col[k] + rank_col[k]) * as_column(rw_ref[k : k + 1, :])
        for k in range(TOPK)
    )
    high = weight.astype(BF16)
    mix_ref[0] = high
    mix_ref[1] = (weight - high.astype(F32)).astype(BF16)

    def block(index):
        return pl.ds(pl.multiple_of(index * CHUNK_ROWS, CHUNK_ROWS), CHUNK_ROWS)

    def group(g, half=None):
        if half is None:
            return pl.ds(pl.multiple_of(g * Z_ROWS, Z_ROWS), Z_ROWS)
        first = Z_ROWS // 2
        if half == 0:
            return pl.ds(pl.multiple_of(g * Z_ROWS, CHUNK_ROWS), first)
        return pl.ds(pl.multiple_of(g * Z_ROWS + first, CHUNK_ROWS), Z_ROWS - first)

    pltpu.make_async_copy(packed.at[block(me)], rows_in.at[x, block(me)], a_recv.at[z]).start()

    def dispatch(n, _):
        where, index = peer(n // 8, lax.rem(n, 8))

        @pl.when(index != me)
        def _():
            send(packed.at[block(index)], rows_in.at[x, block(me)], a_send, a_recv.at[z], where)

        return 0

    lax.fori_loop(0, 64, dispatch, 0)

    for name in ("gate", "up"):
        loads[name].wait()

    def turn(t, _):
        @pl.when(t < NZ)
        def _():
            g = group_of(t)
            ref = rows_in.at[x, group(g)]
            await_(ref, a_recv.at[g])
            for side, other, _origin in sides:
                send(ref, ref, b_send, b_recv.at[side, g], {"tp": other})

        @pl.when((t >= 1) & (t < NZ + 1))
        def _():
            g = group_of(t - 1)
            for side, other, origin in sides:
                await_(rows_in.at[origin, group(g)], b_recv.at[side, g])
                ref = rows_in.at[origin, group(g, side)]
                send(ref, ref, f_send, f_recv.at[side, g], {"tp": other})

        @pl.when((t >= 2) & (t < NZ + 2))
        def _():
            g = group_of(t - 2)
            for side, _other, _origin in sides:
                await_(rows_in.at[across, group(g, side)], f_recv.at[side, g])
            chunks = jnp.concatenate([rows_in[s, group(g)] for s in range(4)], axis=0)
            rows = from_chunks(chunks, swap_ref[...])
            gate = jnp.minimum(jnp.dot(rows, gate_ref[...], preferred_element_type=F32), CLAMP)
            lift = jnp.clip(jnp.dot(rows, up_ref[...], preferred_element_type=F32), -CLAMP, CLAMP)
            active = gate * jax.nn.sigmoid(ALPHA * gate) * (lift + 1.0)
            for s in range(4):
                mine = active[OWN_ROWS * s : OWN_ROWS * s + OWN_ROWS]
                act_out[g, s] = jnp.concatenate([mine[:, :128], mine[:, 128:]], axis=0).astype(BF16)
            act_in[g, x] = act_out[g, x]
            for n, other in enumerate((after, before, across)):
                send(act_out.at[g, other], act_in.at[g, x], g_send, g_recv.at[n, g], {"tp": other})

        @pl.when(t >= 3)
        def _():
            g = group_of(t - 3)

            @pl.when(t == 3)
            def _():
                for side, _other, origin in sides:
                    rest = pl.ds(half_ff * (1 - side), half_ff)
                    await_(down_ref.at[origin, rest], d_recv.at[side, 1 - side])
                    await_(down_ref.at[across, pl.ds(half_ff * side, half_ff)], h_recv.at[side])

            for n, origin in enumerate((before, after, across)):
                await_(act_in.at[g, origin], g_recv.at[n, g])
            lanes = []
            for s in range(4):
                wide = act_in[g, s].astype(F32)
                lanes += [wide[:OWN_ROWS], wide[OWN_ROWS:]]
            acts = jnp.concatenate(lanes, axis=1)
            filler = jnp.zeros((32 - OWN_ROWS, 4 * FF_BLOCK), F32)
            acts = jnp.concatenate([acts, filler], axis=0).astype(BF16)
            down = down_ref[...].reshape(4 * FF_BLOCK, WIDTH)
            result = jnp.dot(acts, down, preferred_element_type=F32).astype(BF16)
            back[group(g)] = to_chunks(result, swap_ref[...])[:Z_ROWS]

            def give(k, _):
                py, pc = lax.rem(y + k // 2, NY), lax.rem(c + k, 2)
                index = (g * NY + py) * 2 + pc

                @pl.when(index == me)
                def _():
                    pltpu.make_async_copy(back.at[block(me)], home.at[block(me)], e_recv.at[z]).start()

                @pl.when(index != me)
                def _():
                    where = {"sp_0": g, "sp_1": py, "sp_2": pc}
                    send(back.at[block(index)], home.at[block(me)], e_send, e_recv.at[z], where)

                return 0

            lax.fori_loop(0, 8, give, 0)

        return 0

    lax.fori_loop(0, NZ + STAGES - 1, turn, 0)

    for g in range(NZ):
        await_(home.at[group(g)], e_recv.at[g])
    results = from_chunks(home[...], swap_ref[...])
    combined = jnp.dot(mix_ref[0], results, preferred_element_type=F32) + jnp.dot(
        mix_ref[1], results, preferred_element_type=F32
    )
    out_ref[...] = (mid_ref[...].astype(F32) + combined).astype(BF16)

    await_(held.at[0, 0, pl.ds(0, NZ - 1)], own_send)
    await_(held.at[0, pl.ds(0, NY - 1)], fwd_send)
    for g in range(NY):
        await_(held.at[c, g], pair_send.at[g])
    await_(down_ref.at[pl.ds(0, 2)], d_send)
    await_(down_ref.at[0], h_send)
    most = pl.ds(0, ALL_ROWS - CHUNK_ROWS)
    await_(packed.at[most], a_send)
    await_(back.at[most], e_send)
    await_(rows_in.at[pl.ds(0, 2)], b_send)
    await_(rows_in.at[0], f_send)
    await_(act_in.at[pl.ds(0, 6)], g_send)


def layer(small, large):
    vmem = pl.BlockSpec(memory_space=pltpu.VMEM)
    anywhere = pl.BlockSpec(memory_space=pl.ANY)
    dma = pltpu.SemaphoreType.DMA
    res, qn, qr, lat, key, upk, upv, ow, gate, up, down = large
    held_in = [
        pltpu.VMEM(a.shape[-2:], BF16) for a in (res, qn, qr, lat, key, upk, upv, ow, gate, up)
    ]
    return pl.pallas_call(
        layer_kernel,
        out_shape=jax.ShapeDtypeStruct(res.shape[1:], BF16),
        in_specs=[anywhere] * (len(small) + len(large)),
        out_specs=vmem,
        scratch_shapes=[pltpu.VMEM(a.shape, a.dtype) for a in small]
        + held_in
        + [
            pltpu.VMEM((4,) + down.shape[1:], BF16),
            pltpu.VMEM((2, NY, NZ, 128, 128), BF16),
            pltpu.VMEM((QROWS, 256), BF16),
            pltpu.VMEM((GROUP, 256), BF16),
            pltpu.VMEM((VROWS, GROUP), BF16),
            pltpu.VMEM((QROWS // CHUNK, GROUP, CHUNK), F32),
            pltpu.VMEM((QROWS // CHUNK, GROUP, CHUNK), BF16),
            pltpu.VMEM((VROWS, QROWS), F32),
            pltpu.VMEM((1, QROWS), F32),
            pltpu.VMEM((TOK, WIDTH), BF16),
            pltpu.VMEM((ALL_ROWS, 128), BF16),
            pltpu.VMEM((4, ALL_ROWS, 128), BF16),
            pltpu.VMEM((NZ, 4, 2 * OWN_ROWS, 128), BF16),
            pltpu.VMEM((NZ, 4, 2 * OWN_ROWS, 128), BF16),
            pltpu.VMEM((ALL_ROWS, 128), BF16),
            pltpu.VMEM((ALL_ROWS, 128), BF16),
            pltpu.VMEM((256, 256), BF16),
            pltpu.VMEM((2, TOK, 2 * TOK), BF16),
            dma((len(small) + len(large),)), dma, dma, dma((NY,)), dma, dma, dma, dma, dma, dma, dma,
            dma((NZ,)), dma((NY, 2)), dma((NY,)), dma((2, 2)), dma((2,)),
            dma((NZ,)), dma((2, NZ)), dma((2, NZ)), dma((3, NZ)), dma((NZ,)),
        ],
        compiler_params=pltpu.CompilerParams(
            collective_id=0, has_side_effects=True, vmem_limit_bytes=60 * 2**20
        ),
    )(*small, *large)


def local(
    residual,
    query_nope,
    query_rope,
    latent,
    rope_key,
    latent_gain,
    up_key,
    up_value,
    out_weight,
    ffn_gain,
    routes,
    route_weight,
    gate_weight,
    up_weight,
    down_weight,
):
    half = ROPE // 2
    inverse = (ROPE_BASE ** (-(np.arange(128) % half) * 2.0 / ROPE)).astype(np.float32)
    small = (
        latent_gain[None],
        ffn_gain[None],
        jnp.asarray(inverse)[None],
        jnp.swapaxes(routes, 1, 2),
        jnp.swapaxes(route_weight[0], 0, 1),
    )
    large = (
        residual, query_nope, query_rope, latent, jnp.swapaxes(rope_key, 1, 2),
        up_key, up_value, out_weight, gate_weight, up_weight, down_weight,
    )
    return layer(small, large)[None]


def solution(mesh):
    split = Mesh(mesh.devices.reshape(8, 4, 2, mesh.shape["tp"]), ("sp_0", "sp_1", "sp_2", "tp"))
    in_specs = (
        P("tp", SP, None),
        P("tp", SP, None),
        P("tp", SP, None),
        P("tp", SP, None),
        P("tp", SP, None),
        P(),
        P(),
        P(),
        P(),
        P(),
        P(None, SP, None),
        P("tp", SP, None),
        P(SP, None, "tp"),
        P(SP, None, "tp"),
        P(SP, "tp", None),
    )
    out_specs = P("tp", SP, None)
    return jax.shard_map(local, mesh=split, in_specs=in_specs, out_specs=out_specs, check_vma=False)
```
